32 devices in a mesh: rep: 2 (over x), fs: 8 (over z, y), tp: 2 (over core).
Axes of the slice: x: 2, y: 2, z: 4, core: 2. Of those that a mesh axis runs over, the one named last changes fastest.
Arguments:
- tokens: bfloat16 [16, 512, 2048], P(('rep', 'fs'), 'tp'), may hold values from -6 to 6
- norm_first: bfloat16 [2048], replicated, may hold values from 0.099609375 to 1.8984375
- norm_mixer: bfloat16 [2048], replicated, may hold values from 0.099609375 to 1.8984375
- norm_second: bfloat16 [2048], replicated, may hold values from 0.099609375 to 1.8984375
- ffn_gate: bfloat16 [2048, 2816], P('fs', 'tp'), may hold values from -0.125 to 0.125
- ffn_up: bfloat16 [2048, 2816], P('fs', 'tp'), may hold values from -0.125 to 0.125
- ffn_down: bfloat16 [2816, 2048], P('tp', 'fs'), may hold values from -0.109375 to 0.109375
- conv_value: bfloat16 [2048, 512], P('fs', 'tp'), may hold values from -0.125 to 0.125
- conv_gate: bfloat16 [2048, 512], P('fs', 'tp'), may hold values from -0.125 to 0.125
- depthwise: bfloat16 [31, 512], P(None, 'tp'), may hold values from -1.5 to 1.5
- conv_gain: bfloat16 [512], P('tp'), may hold values from 0.099609375 to 1.8984375
- conv_out: bfloat16 [512, 2048], P('tp', 'fs'), may hold values from -0.25 to 0.25
Outputs:
- mixed: bfloat16 [16, 512, 2048], P(('rep', 'fs'), 'tp')
The draws below stay inside these ranges and needn't reach their ends.
All inputs are finite; a program needn't handle non-finite values.
Results may differ from the reference program's by a relative error of at most 0.0095.
Values may be sent and summed in bfloat16 or wider, within the bound.
A program may use at most 128 MiB of HBM per device.

```python
import jax
import jax.numpy as jnp
from jax import lax

D = 2048
FF = 2816
CONV = 512
KSIZE = 31
LEN = 512
SEQS = 16
N_TP = 2


def draw_depthwise(key, part):
    first, second, third = jax.random.split(jax.random.fold_in(key, 7), 3)
    base = jnp.clip(jax.random.normal(first, (KSIZE, CONV), jnp.float32), -3.0, 3.0) * KSIZE ** (-0.5)
    flipped = jax.random.randint(second, (), 0, 2)
    channel = jnp.arange(CONV)
    upper = (channel >= CONV // 2).astype(jnp.int32)
    factor = jnp.where(upper == flipped, 0.5, 1.6)
    jitter = jnp.exp(jax.random.uniform(third, (CONV,), jnp.float32, -0.35, 0.35))
    return (base * (factor * jitter)[None, :]).astype(jnp.bfloat16)


def block_levels(rng, extent, cuts, least, high):
    def one(axis_at, shards_of):
        heights = jax.random.uniform(jax.random.fold_in(jax.random.fold_in(rng, 6), axis_at), (shards_of,), jnp.float32, least / len(cuts), high / len(cuts))
        return jnp.repeat(jnp.exp(heights), extent[axis_at] // shards_of).reshape((-1,) + (1,) * (len(extent) - axis_at - 1))

    loudness = one(*cuts[0])
    for cut in cuts[1:]:
        loudness = loudness * one(*cut)
    return loudness


def gaussian(own_key, shape, scale, bound, cuts=(), dtype=jnp.bfloat16):
    result = jax.random.normal(own_key, shape, jnp.float32) * scale
    if len(cuts) > 0:
        result = block_levels(own_key, shape, cuts, -0.22, 0.18) * result
    return jnp.clip(result, min=-bound, max=bound).astype(dtype)


def setup_inputs(seed: int = 0) -> dict:
    arg_keys = jax.random.split(jax.random.key(seed), 13)
    tokens = gaussian(arg_keys[0], (SEQS, LEN, D), 1.0, 6.0, ((0, 16), (1, 2)))
    norm_first = jnp.clip(1.0 + 0.18 * jax.random.normal(arg_keys[1], (D,), jnp.float32), 0.099609375, 1.8984375).astype(jnp.bfloat16)
    norm_mixer = jnp.clip(1.0 + 0.18 * jax.random.normal(arg_keys[2], (D,), jnp.float32), 0.099609375, 1.8984375).astype(jnp.bfloat16)
    norm_second = jnp.clip(1.0 + 0.18 * jax.random.normal(arg_keys[3], (D,), jnp.float32), 0.099609375, 1.8984375).astype(jnp.bfloat16)
    ffn_gate = gaussian(arg_keys[4], (D, FF), D ** -0.5, 0.125, ((0, 8), (1, 2)))
    ffn_up = gaussian(arg_keys[5], (D, FF), D ** -0.5, 0.125, ((0, 8), (1, 2)))
    ffn_down = gaussian(arg_keys[6], (FF, D), FF ** -0.5, 0.109375, ((0, 2), (1, 8)))
    conv_value = gaussian(arg_keys[7], (D, CONV), D ** -0.5, 0.125, ((0, 8), (1, 2)))
    conv_gate = gaussian(arg_keys[8], (D, CONV), D ** -0.5, 0.125, ((0, 8), (1, 2)))
    depthwise = draw_depthwise(jax.random.fold_in(arg_keys[12], 71), 0)
    conv_gain = jnp.clip(1.0 + 0.18 * jax.random.normal(arg_keys[10], (CONV,), jnp.float32), 0.099609375, 1.8984375).astype(jnp.bfloat16)
    conv_out = gaussian(arg_keys[11], (CONV, D), CONV ** -0.5, 0.25, ((0, 2), (1, 8)))
    return {"tokens": tokens, "norm_first": norm_first, "norm_mixer": norm_mixer, "norm_second": norm_second, "ffn_gate": ffn_gate, "ffn_up": ffn_up, "ffn_down": ffn_down, "conv_value": conv_value, "conv_gate": conv_gate, "depthwise": depthwise, "conv_gain": conv_gain, "conv_out": conv_out}


ROW_EPS = 0.05
CHAN_EPS = 0.02

def rms_rows(stream, gain_vec):
    square_mean = lax.optimization_barrier(jnp.mean(stream * stream, axis=-1, keepdims=True))
    return (stream * lax.rsqrt(square_mean + ROW_EPS) * gain_vec.astype(jnp.float32)).astype(jnp.bfloat16)

def block_sum(left, right, blocks):
    width = left.shape[1] // blocks
    running = jnp.zeros((left.shape[0], right.shape[1]), jnp.float32)
    for block in range(blocks):
        partial_value = jnp.dot(left[:, block * width:(block + 1) * width], right[block * width:(block + 1) * width], preferred_element_type=jnp.float32)
        running = running + lax.optimization_barrier(partial_value.astype(jnp.bfloat16)).astype(jnp.float32)
    return running

def causal_taps(glu, kernel):
    length = glu.shape[0]
    padded = jnp.pad(glu, ((KSIZE - 1, 0), (0, 0)))
    output = jnp.zeros_like(glu)
    for tap_index in range(KSIZE):
        output = output + padded[tap_index:tap_index + length] * kernel[tap_index]
    return output

def reference(tokens, norm_first, norm_mixer, norm_second, ffn_gate, ffn_up, ffn_down, conv_value, conv_gate, depthwise, conv_gain, conv_out):

    def feed(normed):
        gate_rows = jnp.dot(normed, ffn_gate, preferred_element_type=jnp.float32)
        up_rows = jnp.dot(normed, ffn_up, preferred_element_type=jnp.float32)
        hidden = (jax.nn.silu(gate_rows) * up_rows).astype(jnp.bfloat16)
        return block_sum(hidden, ffn_down, N_TP)

    def one_sequence(sequence):
        stream = sequence.astype(jnp.float32)
        stream = stream + 0.5 * feed(rms_rows(stream, norm_first))
        normed = rms_rows(stream, norm_mixer)
        values = jnp.dot(normed, conv_value, preferred_element_type=jnp.float32)
        gates = jnp.dot(normed, conv_gate, preferred_element_type=jnp.float32)
        glu = values * jax.nn.sigmoid(gates)
        conv = causal_taps(glu, depthwise.astype(jnp.float32))
        average = lax.optimization_barrier(jnp.mean(conv, axis=-1, keepdims=True))
        centred = conv - average
        spread = lax.optimization_barrier(jnp.mean(centred * centred, axis=-1, keepdims=True))
        activated = jax.nn.silu(centred * lax.rsqrt(spread + CHAN_EPS) * conv_gain.astype(jnp.float32)).astype(jnp.bfloat16)
        stream = stream + block_sum(activated, conv_out, N_TP)
        stream = stream + 0.5 * feed(rms_rows(stream, norm_second))
        return stream.astype(jnp.bfloat16)
    return lax.map(one_sequence, tokens)
```

```python
import functools

import jax
import jax.numpy as jnp
from jax import lax
from jax.experimental import pallas as pl
from jax.experimental.pallas import tpu as pltpu
from jax.sharding import PartitionSpec as P

ROW_EPS = 0.05
CHAN_EPS = 0.02
MESH = pl.DeviceIdType.MESH
CHUNKS = 8
SHARES = ((6, 5), (6, 4), (6, 5), (6, 5))
UP, DOWN, OVER_X, OVER_Y = range(4)


def rms_rows(stream, gain_vec):
    square_mean = jnp.mean(stream * stream, axis=-1, keepdims=True)
    return (stream * lax.rsqrt(square_mean + ROW_EPS) * gain_vec.astype(jnp.float32)).astype(
        jnp.bfloat16
    )


def swap(value):
    size = lax.axis_size("tp")
    return lax.ppermute(value, "tp", [(i, size - 1 - i) for i in range(size)])


def widen(normed):
    return jnp.concatenate([normed, swap(normed)])


def narrow(partial_value):
    rounded = partial_value.astype(jnp.bfloat16)
    half = rounded.shape[0] // 2
    return rounded[:half].astype(jnp.float32) + swap(rounded[half:]).astype(jnp.float32)


def reorder(rows):
    half = rows.shape[0] // 2
    flipped = jnp.concatenate([rows[half:], rows[:half]])
    return jnp.where(lax.axis_index("tp") == 0, rows, flipped)


def place():
    fs = lax.axis_index("fs")
    return lax.axis_index("rep"), lax.rem(fs, 2), fs // 2


class Gather:
    def __init__(self, depth, shares, ins, slots, local_sems, recv_sems, side_sems, send_sems):
        self.depth, self.shares = depth, shares
        self.ins, self.slots = ins, slots
        self.local_sems, self.recv_sems = local_sems, recv_sems
        self.side_sems, self.send_sems = side_sems, send_sems
        self.x, self.y, self.z = place()
        self.has_up, self.has_down = self.z + 1 < depth, self.z > 0
        self.own = self.z * 2 + self.y

    def target(self, way):
        if way == UP:
            return {"fs": (self.z + 1) * 2 + self.y}
        if way == DOWN:
            return {"fs": (self.z - 1) * 2 + self.y}
        if way == OVER_X:
            return {"rep": 1 - self.x}
        return {"fs": self.z * 2 + 1 - self.y}

    def barrier(self):
        barrier = pltpu.get_barrier_semaphore()
        for way in (OVER_X, OVER_Y):
            pl.semaphore_signal(barrier, inc=1, device_id=self.target(way), device_id_type=MESH)
        for way, present in ((UP, self.has_up), (DOWN, self.has_down)):

            @pl.when(present)
            def _(way=way):
                pl.semaphore_signal(barrier, inc=1, device_id=self.target(way), device_id_type=MESH)

        peers = 2 + self.has_up.astype(jnp.int32) + self.has_down.astype(jnp.int32)
        pl.semaphore_wait(barrier, peers)

    def count(self, m):
        return self.slots[m].shape[1]

    def chunk(self, m, e, mine=True):
        count = self.count(m)
        flip = self.x if mine else 1 - self.x
        return e + flip * (count - 1 - 2 * e)

    def chunks(self, m, first, last, mine=True):
        count = self.count(m)
        flip = self.x if mine else 1 - self.x
        return pl.ds(first + flip * (count - last - first), last - first)

    def local(self, m):
        return pltpu.make_async_copy(self.ins[m], self.slots[m].at[self.own], self.local_sems.at[m])

    def copy(self, m, k, c, way):
        piece = self.slots[m].at[k, c]
        recv_sem = self.side_sems[m].at[k] if way == OVER_X else self.recv_sems[m].at[k, c]
        return pltpu.make_async_remote_copy(
            src_ref=piece,
            dst_ref=piece,
            send_sem=self.send_sems[m].at[way, k],
            recv_sem=recv_sem,
            device_id=self.target(way),
            device_id_type=MESH,
        )

    def spread(self, m, k, e, ways):
        c = self.chunk(m, e)
        for way, wanted in ways:
            if wanted is True:
                self.copy(m, k, c, way).start()
            elif wanted is not False:
                pl.when(wanted)(lambda way=way: self.copy(m, k, c, way).start())

    def start_local(self):
        for m in range(len(self.ins)):
            self.local(m).start()

    def start_own(self, m):
        along, across = self.shares[m]
        self.local(m).wait()
        for e in range(along):
            self.spread(m, self.own, e, ((UP, self.has_up), (DOWN, self.has_down), (OVER_Y, e < across)))

    def pieces(self, d):
        return ((self.z - d, self.z - d >= 0, self.has_up, UP), (self.z + d, self.z + d < self.depth, self.has_down, DOWN))

    def arrive_along(self, m, d, e):
        along, across = self.shares[m]
        spare = self.count(m) - along
        for at, present, further, way in self.pieces(d):

            @pl.when(present)
            def _(at=at, further=further, way=way):
                k = at * 2 + self.y
                self.copy(m, k, self.chunk(m, e), UP).wait_recv()
                self.spread(m, k, e, ((way, further), (OVER_Y, e < across), (OVER_X, e < spare)))

    def arrive_across(self, m, d, e):
        spare = self.count(m) - self.shares[m][1]
        for side, (at, present, _, _) in enumerate(self.pieces(d)):
            if side == 1:
                present = jnp.logical_and(present, d > 0)

            @pl.when(present)
            def _(at=at):
                k = at * 2 + 1 - self.y
                self.copy(m, k, self.chunk(m, e), OVER_Y).wait_recv()
                self.spread(m, k, e, ((OVER_X, e < spare),))

    def run(self):
        total = len(self.ins)
        self.start_own(0)
        for m in range(total):
            along, across = self.shares[m]

            def step(r, carry, m=m, along=along, across=across):
                if m + 1 < total:

                    @pl.when(r == max(self.depth - 2, 0))
                    def _():
                        self.start_own(m + 1)

                for e in range(max(along, across)):
                    if e < along:
                        self.arrive_along(m, r + 1, e)
                    if e < across:
                        self.arrive_across(m, r, e)
                return carry

            lax.fori_loop(0, self.depth, step, 0)

    def side(self, m, k, first, last, mine):
        piece = self.slots[m].at[k, self.chunks(m, first, last, mine)]
        return pltpu.make_async_remote_copy(
            src_ref=piece,
            dst_ref=piece,
            send_sem=self.send_sems[m].at[OVER_X, k],
            recv_sem=self.side_sems[m].at[k],
            device_id=self.target(OVER_X),
            device_id_type=MESH,
        )

    def sent(self, m, k, last, way):
        piece = self.slots[m].at[k, self.chunks(m, 0, last)]
        return pltpu.make_async_remote_copy(
            src_ref=piece,
            dst_ref=piece,
            send_sem=self.send_sems[m].at[way, k],
            recv_sem=self.side_sems[m].at[k],
            device_id=self.target(way),
            device_id_type=MESH,
        )

    def drain(self):
        for m in range(len(self.ins)):
            along, across = self.shares[m]
            count = self.count(m)

            def step(d, carry, m=m, along=along, across=across, count=count):
                for side, (at, present, further, way) in enumerate(self.pieces(d)):
                    if side == 1:
                        present = jnp.logical_and(present, d > 0)

                    @pl.when(present)
                    def _(at=at, further=further, way=way):
                        k, cross = at * 2 + self.y, at * 2 + 1 - self.y

                        @pl.when(d > 0)
                        def _():
                            self.side(m, k, 0, count - along, False).wait_recv()
                            self.side(m, k, 0, count - along, True).wait_send()

                        self.side(m, cross, 0, count - across, False).wait_recv()
                        self.side(m, cross, 0, count - across, True).wait_send()
                        self.sent(m, k, across, OVER_Y).wait_send()
                        pl.when(further)(lambda: self.sent(m, k, along, way).wait_send())

                return carry

            lax.fori_loop(0, self.depth, step, 0)

            @pl.when(self.has_down)
            def _(m=m, along=along):
                self.sent(m, self.own, along, DOWN).wait_send()


def gather_kernel(depth, shares, count, *refs):
    ins, slots = refs[:count], refs[count : 2 * count]
    sems = refs[2 * count :]
    local_sems, sems = sems[0], sems[1:]
    gather = Gather(depth, shares, ins, slots, local_sems, sems[:count], sems[count : 2 * count], sems[2 * count :])
    gather.start_local()
    gather.barrier()
    gather.run()
    gather.drain()


def gather_all(blocks, shares):
    total = lax.axis_size("fs")
    count = len(blocks)
    outs = [jax.ShapeDtypeStruct((total, *b.shape), b.dtype) for b in blocks]
    dma = pltpu.SemaphoreType.DMA
    return pl.pallas_call(
        functools.partial(gather_kernel, total // 2, shares, count),
        out_shape=outs,
        in_specs=[pl.BlockSpec(memory_space=pl.ANY)] * count,
        out_specs=[pl.BlockSpec(memory_space=pltpu.VMEM)] * count,
        scratch_shapes=[dma((count,))]
        + [dma((total, b.shape[0])) for b in blocks]
        + [dma((total,)) for b in blocks]
        + [dma((4, total)) for b in blocks],
        compiler_params=pltpu.CompilerParams(
            collective_id=0, has_side_effects=True, vmem_limit_bytes=48 * 2**20
        ),
        name="gather_all",
    )(*blocks)


def hidden_units(gathered, whole_gate, whole_up):
    gate_rows = jnp.dot(gathered, whole_gate, preferred_element_type=jnp.float32)
    up_rows = jnp.dot(gathered, whole_up, preferred_element_type=jnp.float32)
    return (jax.nn.silu(gate_rows) * up_rows).astype(jnp.bfloat16)


def columns_of(blocks):
    return blocks.transpose(1, 0, 2).reshape(blocks.shape[1], -1)


def causal_taps(glu, kernel):
    length = glu.shape[0]
    taps = kernel.shape[0]
    padded = jnp.pad(glu, ((taps - 1, 0), (0, 0)))
    output = jnp.zeros_like(glu)
    for tap_index in range(taps):
        output = output + padded[tap_index : tap_index + length] * kernel[tap_index]
    return output


def chunked(block, pieces):
    return block.reshape(pieces, block.shape[0] // pieces, block.shape[1])


def shards(
    tokens,
    norm_first,
    norm_mixer,
    norm_second,
    ffn_gate,
    ffn_up,
    ffn_down,
    conv_value,
    conv_gate,
    depthwise,
    conv_gain,
    conv_out,
):
    width = tokens.shape[-1]
    stream = tokens.reshape(-1, width).astype(jnp.float32)
    first_rows = widen(rms_rows(stream, norm_first))
    small = jnp.concatenate([conv_value, conv_gate, conv_out.reshape(-1, conv_value.shape[1])])
    gate, up, down, small_all = gather_all(
        [chunked(block, CHUNKS) for block in (ffn_gate, ffn_up, ffn_down, small)], SHARES
    )
    whole_gate = gate.reshape(-1, gate.shape[-1])
    whole_up = up.reshape(-1, up.shape[-1])
    whole_down = columns_of(down.reshape(down.shape[0], -1, down.shape[-1]))
    total = small_all.shape[0]
    small_all = small_all.reshape(total, -1, small_all.shape[-1])
    rows = conv_value.shape[0]
    channels_here = conv_value.shape[1]
    whole_value = small_all[:, :rows].reshape(-1, channels_here)
    whole_conv_gate = small_all[:, rows : 2 * rows].reshape(-1, channels_here)
    whole_out = columns_of(small_all[:, 2 * rows :].reshape(total, *conv_out.shape))

    hidden = hidden_units(first_rows, whole_gate, whole_up)
    stream = stream + 0.5 * narrow(jnp.dot(hidden, whole_down, preferred_element_type=jnp.float32))
    gathered = widen(rms_rows(stream, norm_mixer))
    values = jnp.dot(gathered, whole_value, preferred_element_type=jnp.float32)
    gates = jnp.dot(gathered, whole_conv_gate, preferred_element_type=jnp.float32)
    glu = reorder(values * jax.nn.sigmoid(gates))
    conv = causal_taps(glu, depthwise.astype(jnp.float32))
    channels = conv.shape[1] * lax.axis_size("tp")
    sums, squares = lax.psum((jnp.sum(conv, axis=1), jnp.sum(conv * conv, axis=1)), "tp")
    average = sums / channels
    spread = jnp.maximum(squares / channels - average * average, 0.0)
    centred = conv - average[:, None]
    activated = jax.nn.silu(
        centred * lax.rsqrt(spread[:, None] + CHAN_EPS) * conv_gain.astype(jnp.float32)
    ).astype(jnp.bfloat16)
    stream = stream + narrow(jnp.dot(reorder(activated), whole_out, preferred_element_type=jnp.float32))
    second_rows = widen(rms_rows(stream, norm_second))
    second_hidden = hidden_units(second_rows, whole_gate, whole_up)
    stream = stream + 0.5 * narrow(jnp.dot(second_hidden, whole_down, preferred_element_type=jnp.float32))
    return stream.astype(jnp.bfloat16).reshape(tokens.shape)


def solution(mesh):
    in_specs = (
        P(("rep", "fs"), "tp", None),
        P(),
        P(),
        P(),
        P("fs", "tp"),
        P("fs", "tp"),
        P("tp", "fs"),
        P("fs", "tp"),
        P("fs", "tp"),
        P(None, "tp"),
        P("tp"),
        P("tp", "fs"),
    )
    out_specs = P(("rep", "fs"), "tp", None)
    return jax.shard_map(shards, mesh=mesh, in_specs=in_specs, out_specs=out_specs, check_vma=False)
```

```python
import functools

import jax
import jax.numpy as jnp
from jax import lax
from jax.experimental import pallas as pl
from jax.experimental.pallas import tpu as pltpu
from jax.sharding import PartitionSpec as P

ROW_EPS = 0.05
CHAN_EPS = 0.02
MESH = pl.DeviceIdType.MESH
CHUNKS = 8
LANES = 128
ROW_BLOCK = 32
CONV_BLOCK = 64
PAD = 32
FIRST_SLOT = 6
SECOND_SLOT = 4
SHARES = ((6, 5), (6, 4), (6, 5), (6, 5))
UP, DOWN, OVER_X, OVER_Y = range(4)


def rms_rows(stream, gain_vec):
    square_mean = jnp.mean(stream * stream, axis=-1, keepdims=True)
    return (stream * lax.rsqrt(square_mean + ROW_EPS) * gain_vec.astype(jnp.float32)).astype(
        jnp.bfloat16
    )


def swap(value):
    size = lax.axis_size("tp")
    return lax.ppermute(value, "tp", [(i, size - 1 - i) for i in range(size)])


def widen(normed):
    return jnp.concatenate([normed, swap(normed)])


def narrow(partial_value):
    rounded = partial_value.astype(jnp.bfloat16)
    half = rounded.shape[0] // 2
    return rounded[:half].astype(jnp.float32) + swap(rounded[half:]).astype(jnp.float32)


def reorder(rows):
    half = rows.shape[0] // 2
    flipped = jnp.concatenate([rows[half:], rows[:half]])
    return jnp.where(lax.axis_index("tp") == 0, rows, flipped)


def place():
    fs = lax.axis_index("fs")
    return lax.axis_index("rep"), lax.rem(fs, 2), fs // 2


class Gather:
    def __init__(self, depth, shares, ins, slots, local_sems, recv_sems, side_sems, send_sems):
        self.depth, self.shares = depth, shares
        self.ins, self.slots = ins, slots
        self.local_sems, self.recv_sems = local_sems, recv_sems
        self.side_sems, self.send_sems = side_sems, send_sems
        self.x, self.y, self.z = place()
        self.has_up, self.has_down = self.z + 1 < depth, self.z > 0
        self.own = self.z * 2 + self.y

    def target(self, way):
        if way == UP:
            return {"fs": (self.z + 1) * 2 + self.y}
        if way == DOWN:
            return {"fs": (self.z - 1) * 2 + self.y}
        if way == OVER_X:
            return {"rep": 1 - self.x}
        return {"fs": self.z * 2 + 1 - self.y}

    def barrier(self, *others):
        barrier = pltpu.get_barrier_semaphore()
        for target in (self.target(OVER_X), self.target(OVER_Y), *others):
            pl.semaphore_signal(barrier, inc=1, device_id=target, device_id_type=MESH)
        for way, present in ((UP, self.has_up), (DOWN, self.has_down)):

            @pl.when(present)
            def _(way=way):
                pl.semaphore_signal(barrier, inc=1, device_id=self.target(way), device_id_type=MESH)

        peers = 2 + len(others) + self.has_up.astype(jnp.int32) + self.has_down.astype(jnp.int32)
        pl.semaphore_wait(barrier, peers)

    def count(self, m):
        return self.slots[m].shape[1]

    def chunk(self, m, e, mine=True):
        count = self.count(m)
        flip = self.x if mine else 1 - self.x
        return e + flip * (count - 1 - 2 * e)

    def chunks(self, m, first, last, mine=True):
        count = self.count(m)
        flip = self.x if mine else 1 - self.x
        return pl.ds(first + flip * (count - last - first), last - first)

    def locals(self, m):
        copies, first = [], 0
        for n, part in enumerate(self.ins[m]):
            height = part.shape[1]
            here = self.slots[m].at[self.own, :, pl.ds(first, height)]
            copies.append(pltpu.make_async_copy(part, here, self.local_sems.at[m, n]))
            first += height
        return copies

    def copy(self, m, k, c, way):
        piece = self.slots[m].at[k, c]
        recv_sem = self.side_sems[m].at[k] if way == OVER_X else self.recv_sems[m].at[k, c]
        return pltpu.make_async_remote_copy(
            src_ref=piece,
            dst_ref=piece,
            send_sem=self.send_sems[m].at[way, k],
            recv_sem=recv_sem,
            device_id=self.target(way),
            device_id_type=MESH,
        )

    def spread(self, m, k, e, ways):
        c = self.chunk(m, e)
        for way, wanted in ways:
            pl.when(wanted)(lambda way=way: self.copy(m, k, c, way).start())

    def start_local(self):
        for m in range(len(self.ins)):
            for part in self.locals(m):
                part.start()

    def start_own(self, m):
        along, across = self.shares[m]
        for part in self.locals(m):
            part.wait()

        def step(e, carry):
            self.spread(m, self.own, e, ((UP, self.has_up), (DOWN, self.has_down), (OVER_Y, e < across)))
            return carry

        lax.fori_loop(0, along, step, 0)

    def pieces(self, d):
        return ((self.z - d, self.z - d >= 0, self.has_up, UP), (self.z + d, self.z + d < self.depth, self.has_down, DOWN))

    def arrive_along(self, m, d, e):
        along, across = self.shares[m]
        spare = self.count(m) - along
        for at, present, further, way in self.pieces(d):

            @pl.when(present)
            def _(at=at, further=further, way=way):
                k = at * 2 + self.y
                self.copy(m, k, self.chunk(m, e), UP).wait_recv()
                self.spread(m, k, e, ((way, further), (OVER_Y, e < across), (OVER_X, e < spare)))

    def arrive_across(self, m, d, e):
        spare = self.count(m) - self.shares[m][1]
        for side, (at, present, _, _) in enumerate(self.pieces(d)):
            if side == 1:
                present = jnp.logical_and(present, d > 0)

            @pl.when(present)
            def _(at=at):
                k = at * 2 + 1 - self.y
                self.copy(m, k, self.chunk(m, e), OVER_Y).wait_recv()
                self.spread(m, k, e, ((OVER_X, e < spare),))

    def slots_of(self, m):
        return self.depth * self.shares[m][0]

    def run(self, m, work=None):
        along, across = self.shares[m]
        ahead = max(self.depth - 2, 0) * along

        def step(t, carry):
            r, e = lax.div(t, along), lax.rem(t, along)
            if m + 1 < len(self.ins):
                pl.when(t == ahead)(lambda: self.start_own(m + 1))
            self.arrive_along(m, r + 1, e)
            pl.when(e < across)(lambda: self.arrive_across(m, r, e))
            if work is not None:
                work(t)
            return carry

        lax.fori_loop(0, self.slots_of(m), step, 0)

    def side(self, m, k, first, last, mine):
        piece = self.slots[m].at[k, self.chunks(m, first, last, mine)]
        return pltpu.make_async_remote_copy(
            src_ref=piece,
            dst_ref=piece,
            send_sem=self.send_sems[m].at[OVER_X, k],
            recv_sem=self.side_sems[m].at[k],
            device_id=self.target(OVER_X),
            device_id_type=MESH,
        )

    def sent(self, m, k, last, way):
        piece = self.slots[m].at[k, self.chunks(m, 0, last)]
        return pltpu.make_async_remote_copy(
            src_ref=piece,
            dst_ref=piece,
            send_sem=self.send_sems[m].at[way, k],
            recv_sem=self.side_sems[m].at[k],
            device_id=self.target(way),
            device_id_type=MESH,
        )

    def every(self, visit):
        def step(d, carry):
            for side, (at, present, further, way) in enumerate(self.pieces(d)):
                if side == 1:
                    present = jnp.logical_and(present, d > 0)
                pl.when(present)(lambda at=at, further=further, way=way: visit(d, at, further, way))
            return carry

        lax.fori_loop(0, self.depth, step, 0)

    def settle(self, m):
        along, across = self.shares[m]
        count = self.count(m)

        def visit(d, at, further, way):
            k, cross = at * 2 + self.y, at * 2 + 1 - self.y
            pl.when(d > 0)(lambda: self.side(m, k, 0, count - along, False).wait_recv())
            self.side(m, cross, 0, count - across, False).wait_recv()

        self.every(visit)

    def drain(self, m):
        along, across = self.shares[m]
        count = self.count(m)

        def visit(d, at, further, way):
            k, cross = at * 2 + self.y, at * 2 + 1 - self.y
            pl.when(d > 0)(lambda: self.side(m, k, 0, count - along, True).wait_send())
            self.side(m, cross, 0, count - across, True).wait_send()
            self.sent(m, k, across, OVER_Y).wait_send()
            pl.when(further)(lambda: self.sent(m, k, along, way).wait_send())

        self.every(visit)
        pl.when(self.has_down)(lambda: self.sent(m, self.own, along, DOWN).wait_send())


def gather_sems(total, parts, counts):
    dma = pltpu.SemaphoreType.DMA
    return (
        [dma((len(counts), parts))]
        + [dma((total, count)) for count in counts]
        + [dma((total,)) for _ in counts]
        + [dma((4, total)) for _ in counts]
    )


def gather_kernel(depth, shares, count, *refs):
    ins, slots = [(ref,) for ref in refs[:count]], refs[count : 2 * count]
    sems = refs[2 * count :]
    gather = Gather(depth, shares, ins, slots, sems[0], *(sems[1 + i * count : 1 + (i + 1) * count] for i in range(3)))
    gather.start_local()
    gather.barrier()
    gather.start_own(0)
    for m in range(count):
        gather.run(m)
    for m in range(count):
        gather.settle(m)
        gather.drain(m)


def gather_all(blocks, shares):
    total = lax.axis_size("fs")
    count = len(blocks)
    outs = [jax.ShapeDtypeStruct((total, *b.shape), b.dtype) for b in blocks]
    return pl.pallas_call(
        functools.partial(gather_kernel, total // 2, shares, count),
        out_shape=outs,
        in_specs=[pl.BlockSpec(memory_space=pl.ANY)] * count,
        out_specs=[pl.BlockSpec(memory_space=pltpu.VMEM)] * count,
        scratch_shapes=gather_sems(total, 1, [b.shape[0] for b in blocks]),
        compiler_params=pltpu.CompilerParams(
            collective_id=0, has_side_effects=True, vmem_limit_bytes=48 * 2**20
        ),
        name="gather_all",
    )(*blocks)


def hidden_units(gathered, whole_gate, whole_up):
    gate_rows = jnp.dot(gathered, whole_gate, preferred_element_type=jnp.float32)
    up_rows = jnp.dot(gathered, whole_up, preferred_element_type=jnp.float32)
    return (jax.nn.silu(gate_rows) * up_rows).astype(jnp.bfloat16)


def columns_of(blocks):
    return blocks.transpose(1, 0, 2).reshape(blocks.shape[1], -1)


def causal_taps(glu, kernel):
    length = glu.shape[0]
    taps = kernel.shape[0]
    padded = jnp.pad(glu, ((taps - 1, 0), (0, 0)))
    output = jnp.zeros_like(glu)
    for tap_index in range(taps):
        output = output + padded[tap_index : tap_index + length] * kernel[tap_index]
    return output


def chunked(block, pieces):
    return block.reshape(pieces, block.shape[0] // pieces, block.shape[1])


class Layer:
    def __init__(self, gather, tokens, gains, taps, gain, out, scratch):
        self.gather = gather
        self.tokens, self.gains, self.taps, self.gain, self.out = tokens, gains, taps, gain, out
        (
            self.own,
            self.stream,
            self.rows,
            self.hidden,
            self.partial,
            self.landed,
            self.padded,
            self.conv,
            self.sums,
            self.act,
            self.own_sem,
            self.row_send,
            self.row_recv,
            self.part_send,
            self.part_recv,
            self.sum_send,
            self.sum_recv,
        ) = scratch
        self.half, self.width = self.own.shape
        self.units = self.hidden.shape[1]
        self.total = gather.depth * 2
        self.piece = self.width // self.total
        self.tp = lax.axis_index("tp")
        self.partner = {"tp": 1 - self.tp}
        self.mine = pl.multiple_of(self.tp * self.half, self.half)
        self.theirs = pl.multiple_of((1 - self.tp) * self.half, self.half)

    def remote(self, src, dst, send_sem, recv_sem):
        return pltpu.make_async_remote_copy(
            src_ref=src,
            dst_ref=dst,
            send_sem=send_sem,
            recv_sem=recv_sem,
            device_id=self.partner,
            device_id_type=MESH,
        )

    def row_copy(self, n, start=None):
        here = self.rows.at[n, pl.ds(self.mine if start is None else start, self.half)]
        return self.remote(here, here, self.row_send.at[n], self.row_recv.at[n])

    def part_copy(self, n, k):
        cols = pl.ds(pl.multiple_of(k * self.piece, self.piece), self.piece)
        return self.remote(
            self.partial.at[n, pl.ds(self.theirs, self.half), cols],
            self.landed.at[n, :, cols],
            self.part_send.at[n, k],
            self.part_recv.at[n, k],
        )

    def sum_copy(self):
        return self.remote(self.sums.at[0], self.sums.at[1], self.sum_send.at[0], self.sum_recv.at[0])

    def norm(self, n, first, stream):
        square_mean = jnp.mean(stream * stream, axis=-1, keepdims=True)
        scaled = stream * lax.rsqrt(square_mean + ROW_EPS) * self.gains[n][...].astype(jnp.float32)
        self.rows[n, pl.ds(self.mine + first, stream.shape[0]), :] = scaled.astype(jnp.bfloat16)

    def block(self, i):
        return pl.multiple_of(i * ROW_BLOCK, ROW_BLOCK)

    def start_rows(self):
        def step(i, carry):
            first = self.block(i)
            self.norm(0, first, self.own[pl.ds(first, ROW_BLOCK), :].astype(jnp.float32))
            return carry

        lax.fori_loop(0, self.half // ROW_BLOCK, step, 0)
        self.row_copy(0).start()

    def update(self, n, i, scale):
        first = self.block(i)
        here = pl.ds(first, ROW_BLOCK)
        before = self.own[here, :].astype(jnp.float32) if n == 0 else self.stream[here, :]
        added = self.partial[n, pl.ds(self.mine + first, ROW_BLOCK), :].astype(jnp.float32) + self.landed[
            n, here, :
        ].astype(jnp.float32)
        stream = before + (added if scale is None else scale * added)
        self.stream[here, :] = stream
        self.norm(n + 1, first, stream)

    def await_parts(self, n):
        def step(k, carry):
            self.part_copy(n, k).wait_recv()
            return carry

        lax.fori_loop(0, self.total, step, 0)

    def matrix(self, m, first, size):
        return self.gather.slots[m][:, :, :, pl.ds(first, size)].reshape(self.width, size)

    def hidden_tile(self, n, row, height, first, size):
        rows = self.rows[n, pl.ds(row, height), :]
        gate = jnp.dot(rows, self.matrix(0, first, size), preferred_element_type=jnp.float32)
        up = jnp.dot(rows, self.matrix(1, first, size), preferred_element_type=jnp.float32)
        self.hidden[pl.ds(row, height), pl.ds(first, size)] = (jax.nn.silu(gate) * up).astype(jnp.bfloat16)

    def down_piece(self, n, k):
        weights = self.gather.slots[2][k].reshape(self.units, self.piece)
        result = jnp.dot(self.hidden[...], weights, preferred_element_type=jnp.float32)
        cols = pl.ds(pl.multiple_of(k * self.piece, self.piece), self.piece)
        self.partial[n, :, cols] = result.astype(jnp.bfloat16)
        self.part_copy(n, k).start()

    def first_work(self, t):
        j = t - FIRST_SLOT

        @pl.when(j == 0)
        def _():
            self.gather.settle(0)
            self.gather.settle(1)
            self.row_copy(0, self.theirs).wait_recv()

        @pl.when(jnp.logical_and(j >= 0, j < self.units // LANES))
        def _():
            self.hidden_tile(0, 0, 2 * self.half, pl.multiple_of(j * LANES, LANES), LANES)

    def second_work(self, t):
        j = t - SECOND_SLOT
        blocks = self.half // ROW_BLOCK
        i = j - self.total
        pl.when(j == 0)(lambda: self.gather.settle(2))
        pl.when(jnp.logical_and(j >= 0, i < 0))(lambda: self.down_piece(0, j))
        pl.when(i == 0)(lambda: self.await_parts(0))
        pl.when(jnp.logical_and(i >= 0, i < blocks))(lambda: self.update(0, i, 0.5))
        pl.when(i == blocks - 1)(lambda: self.row_copy(1).start())

    def small(self, n):
        height = self.gather.slots[3].shape[2] // 3
        return (pl.ds(n * height, height),)

    def gated(self, row):
        rows = self.rows[1, pl.ds(row, self.half), :]
        value_at, gate_at = self.small(0)[0], self.small(1)[0]
        whole = self.gather.slots[3]
        value = whole[:, :, value_at, :].reshape(self.width, -1)
        gate = whole[:, :, gate_at, :].reshape(self.width, -1)
        values = jnp.dot(rows, value, preferred_element_type=jnp.float32)
        gates = jnp.dot(rows, gate, preferred_element_type=jnp.float32)
        self.padded[pl.ds(PAD + row, self.half), :] = values * jax.nn.sigmoid(gates)

    def convolve(self):
        taps = self.taps.shape[0]
        lanes = self.sums.shape[-1]

        def step(i, carry):
            first = pl.multiple_of(i * CONV_BLOCK, CONV_BLOCK)
            window = self.padded[pl.ds(first, CONV_BLOCK + PAD), :]
            total = jnp.zeros((CONV_BLOCK, window.shape[1]), jnp.float32)
            for j in range(taps):
                at = PAD - (taps - 1) + j
                total = total + window[at : at + CONV_BLOCK] * self.taps[j : j + 1, :].astype(jnp.float32)
            here = pl.ds(first, CONV_BLOCK)
            self.conv[here, :] = total
            plain = jnp.sum(total, axis=-1, keepdims=True)
            squared = jnp.sum(total * total, axis=-1, keepdims=True)
            lane = lax.broadcasted_iota(jnp.int32, (CONV_BLOCK, lanes), 1)
            self.sums[0, here, :] = jnp.where(lane < lanes // 2, plain, squared)
            return carry

        lax.fori_loop(0, 2 * self.half // CONV_BLOCK, step, 0)

    def activate(self):
        lanes = self.sums.shape[-1]
        channels = 2 * self.conv.shape[1]

        def step(i, carry):
            here = pl.ds(pl.multiple_of(i * CONV_BLOCK, CONV_BLOCK), CONV_BLOCK)
            sums = (self.sums[0, here, :] + self.sums[1, here, :]) / channels
            average, square = sums[:, :1], sums[:, lanes // 2 : lanes // 2 + 1]
            spread = jnp.maximum(square - average * average, 0.0)
            scaled = (self.conv[here, :] - average) * lax.rsqrt(spread + CHAN_EPS) * self.gain[...].astype(jnp.float32)
            self.act[here, :] = jax.nn.silu(scaled).astype(jnp.bfloat16)
            return carry

        lax.fori_loop(0, 2 * self.half // CONV_BLOCK, step, 0)

    def mix(self):
        at = self.small(2)[0]

        def step(k, carry):
            weights = self.gather.slots[3][k, :, at, :].reshape(-1, self.piece)
            result = jnp.dot(self.act[...], weights, preferred_element_type=jnp.float32)
            cols = pl.ds(pl.multiple_of(k * self.piece, self.piece), self.piece)
            self.partial[1, :, cols] = result.astype(jnp.bfloat16)
            self.part_copy(1, k).start()
            return carry

        lax.fori_loop(0, self.total, step, 0)

    def conv_module(self):
        self.padded[:PAD, :] = jnp.zeros((PAD, self.padded.shape[1]), jnp.float32)
        self.gated(self.mine)
        self.row_copy(1, self.theirs).wait_recv()
        self.gated(self.theirs)
        self.convolve()
        self.sum_copy().start()
        self.sum_copy().wait_recv()
        self.activate()
        self.mix()
        self.await_parts(1)

        def step(i, carry):
            self.update(1, i, None)
            return carry

        lax.fori_loop(0, self.half // ROW_BLOCK, step, 0)
        self.row_copy(2).start()

    def second_half_step(self):
        tile = 2 * LANES
        whole = self.units // tile
        early = min(2, whole)

        def split(i, carry):
            pl.when(i == early)(lambda: self.row_copy(2, self.theirs).wait_recv())
            row = jnp.where(i < early, self.mine, self.theirs)
            first = pl.multiple_of(lax.rem(i, early) * tile, tile)
            self.hidden_tile(2, pl.multiple_of(row, self.half), self.half, first, tile)
            return carry

        lax.fori_loop(0, 2 * early, split, 0)

        def step(j, carry):
            self.hidden_tile(2, 0, 2 * self.half, pl.multiple_of(j * tile, tile), tile)
            return carry

        lax.fori_loop(early, whole, step, 0)
        if self.units % tile:
            self.hidden_tile(2, 0, 2 * self.half, whole * tile, self.units % tile)

        def piece(k, carry):
            self.down_piece(2, k)
            return carry

        lax.fori_loop(0, self.total, piece, 0)

        def finish(k, carry):
            self.part_copy(2, k).wait_recv()
            cols = pl.ds(pl.multiple_of(k * self.piece, self.piece), self.piece)
            added = self.partial[2, pl.ds(self.mine, self.half), cols].astype(jnp.float32) + self.landed[
                2, :, cols
            ].astype(jnp.float32)
            self.out[:, cols] = (self.stream[:, cols] + 0.5 * added).astype(self.out.dtype)
            return carry

        lax.fori_loop(0, self.total, finish, 0)

    def run(self):
        gather = self.gather
        own = pltpu.make_async_copy(self.tokens, self.own, self.own_sem.at[0])
        gather.start_local()
        own.start()
        gather.barrier(self.partner)
        gather.start_own(0)
        own.wait()
        self.start_rows()
        gather.run(0)
        gather.run(1)
        gather.run(2, self.first_work)
        gather.run(3, self.second_work)
        gather.settle(3)
        self.conv_module()
        self.second_half_step()
        for m in range(len(gather.ins)):
            gather.drain(m)
        self.sum_copy().wait_send()

        def step(n, carry):
            self.row_copy(n).wait_send()

            def piece(k, inner):
                self.part_copy(n, k).wait_send()
                return inner

            return lax.fori_loop(0, self.total, piece, carry)

        lax.fori_loop(0, 3, step, 0)


def layer_kernel(depth, *refs):
    tokens, gains, refs = refs[0], refs[1:4], refs[4:]
    ins, refs = ((refs[0],), (refs[1],), (refs[2],), refs[3:6]), refs[6:]
    taps, gain, out, refs = refs[0], refs[1], refs[2], refs[3:]
    slots, sems, scratch = refs[:4], refs[4:17], refs[17:]
    gather = Gather(depth, SHARES, ins, slots, sems[0], sems[1:5], sems[5:9], sems[9:13])
    Layer(gather, tokens, gains, taps, gain, out, scratch).run()


def fused_layer(tokens, gains, blocks, smalls, depthwise, conv_gain):
    total = lax.axis_size("fs")
    half, width = tokens.shape
    units, channels = blocks[0].shape[2], depthwise.shape[1]
    vmem, dma = pltpu.VMEM, pltpu.SemaphoreType.DMA
    merged = (smalls[0].shape[0], 3 * smalls[0].shape[1], smalls[0].shape[2])
    shapes = [b.shape for b in blocks] + [merged]
    f32, bf16 = jnp.float32, jnp.bfloat16
    any_space, in_vmem = pl.BlockSpec(memory_space=pl.ANY), pl.BlockSpec(memory_space=pltpu.VMEM)
    return pl.pallas_call(
        functools.partial(layer_kernel, total // 2),
        out_shape=jax.ShapeDtypeStruct((half, width), bf16),
        in_specs=[any_space] + [in_vmem] * 3 + [any_space] * 6 + [in_vmem] * 2,
        out_specs=in_vmem,
        scratch_shapes=[vmem((total, *shape), bf16) for shape in shapes]
        + gather_sems(total, 3, [shape[0] for shape in shapes])
        + [
            vmem((half, width), bf16),
            vmem((half, width), f32),
            vmem((3, 2 * half, width), bf16),
            vmem((2 * half, units), bf16),
            vmem((3, 2 * half, width), bf16),
            vmem((3, half, width), bf16),
            vmem((PAD + 2 * half, channels), f32),
            vmem((2 * half, channels), f32),
            vmem((2, 2 * half, LANES), f32),
            vmem((2 * half, channels), bf16),
            dma((1,)),
            dma((3,)),
            dma((3,)),
            dma((3, total)),
            dma((3, total)),
            dma((1,)),
            dma((1,)),
        ],
        compiler_params=pltpu.CompilerParams(
            collective_id=0, has_side_effects=True, vmem_limit_bytes=60 * 2**20
        ),
        name="fused_layer",
    )(tokens, *gains, *blocks, *smalls, depthwise, conv_gain)


def fits(half, ffn_gate, ffn_down, conv_value, conv_out, depthwise):
    piece, total = ffn_gate.shape[0], lax.axis_size("fs")
    slots = total // 2 * SHARES[0][0]
    return (
        piece % (16 * CHUNKS) == 0
        and ffn_down.shape[0] % (16 * CHUNKS) == 0
        and conv_out.shape[0] == piece
        and conv_value.shape[1] == piece
        and piece % LANES == 0
        and ffn_gate.shape[1] % LANES == 0
        and half % ROW_BLOCK == 0
        and half % CONV_BLOCK == 0
        and depthwise.shape[0] <= PAD
        and slots >= FIRST_SLOT + ffn_gate.shape[1] // LANES
        and slots >= SECOND_SLOT + total + half // ROW_BLOCK
        and lax.axis_size("tp") == 2
        and lax.axis_size("rep") == 2
    )


def shards(
    tokens,
    norm_first,
    norm_mixer,
    norm_second,
    ffn_gate,
    ffn_up,
    ffn_down,
    conv_value,
    conv_gate,
    depthwise,
    conv_gain,
    conv_out,
):
    width = tokens.shape[-1]
    if fits(tokens.size // width, ffn_gate, ffn_down, conv_value, conv_out, depthwise):
        mixed = fused_layer(
            tokens.reshape(-1, width),
            [gain.reshape(1, -1) for gain in (norm_first, norm_mixer, norm_second)],
            [chunked(block, CHUNKS) for block in (ffn_gate, ffn_up, ffn_down)],
            [chunked(block, CHUNKS) for block in (conv_value, conv_gate, conv_out)],
            depthwise,
            conv_gain.reshape(1, -1),
        )
        return mixed.reshape(tokens.shape)
    stream = tokens.reshape(-1, width).astype(jnp.float32)
    first_rows = widen(rms_rows(stream, norm_first))
    small = jnp.concatenate([conv_value, conv_gate, conv_out.reshape(-1, conv_value.shape[1])])
    gate, up, down, small_all = gather_all(
        [chunked(block, CHUNKS) for block in (ffn_gate, ffn_up, ffn_down, small)], SHARES
    )
    whole_gate = gate.reshape(-1, gate.shape[-1])
    whole_up = up.reshape(-1, up.shape[-1])
    whole_down = columns_of(down.reshape(down.shape[0], -1, down.shape[-1]))
    total = small_all.shape[0]
    small_all = small_all.reshape(total, -1, small_all.shape[-1])
    rows = conv_value.shape[0]
    channels_here = conv_value.shape[1]
    whole_value = small_all[:, :rows].reshape(-1, channels_here)
    whole_conv_gate = small_all[:, rows : 2 * rows].reshape(-1, channels_here)
    whole_out = columns_of(small_all[:, 2 * rows :].reshape(total, *conv_out.shape))

    hidden = hidden_units(first_rows, whole_gate, whole_up)
    stream = stream + 0.5 * narrow(jnp.dot(hidden, whole_down, preferred_element_type=jnp.float32))
    gathered = widen(rms_rows(stream, norm_mixer))
    values = jnp.dot(gathered, whole_value, preferred_element_type=jnp.float32)
    gates = jnp.dot(gathered, whole_conv_gate, preferred_element_type=jnp.float32)
    glu = reorder(values * jax.nn.sigmoid(gates))
    conv = causal_taps(glu, depthwise.astype(jnp.float32))
    channels = conv.shape[1] * lax.axis_size("tp")
    sums, squares = lax.psum((jnp.sum(conv, axis=1), jnp.sum(conv * conv, axis=1)), "tp")
    average = sums / channels
    spread = jnp.maximum(squares / channels - average * average, 0.0)
    centred = conv - average[:, None]
    activated = jax.nn.silu(
        centred * lax.rsqrt(spread[:, None] + CHAN_EPS) * conv_gain.astype(jnp.float32)
    ).astype(jnp.bfloat16)
    stream = stream + narrow(jnp.dot(reorder(activated), whole_out, preferred_element_type=jnp.float32))
    second_rows = widen(rms_rows(stream, norm_second))
    second_hidden = hidden_units(second_rows, whole_gate, whole_up)
    stream = stream + 0.5 * narrow(jnp.dot(second_hidden, whole_down, preferred_element_type=jnp.float32))
    return stream.astype(jnp.bfloat16).reshape(tokens.shape)


def solution(mesh):
    in_specs = (
        P(("rep", "fs"), "tp", None),
        P(),
        P(),
        P(),
        P("fs", "tp"),
        P("fs", "tp"),
        P("tp", "fs"),
        P("fs", "tp"),
        P("fs", "tp"),
        P(None, "tp"),
        P("tp"),
        P("tp", "fs"),
    )
    out_specs = P(("rep", "fs"), "tp", None)
    return jax.shard_map(shards, mesh=mesh, in_specs=in_specs, out_specs=out_specs, check_vma=False)
```

```python
import functools

import jax
import jax.numpy as jnp
from jax import lax
from jax.experimental import pallas as pl
from jax.experimental.pallas import tpu as pltpu
from jax.sharding import PartitionSpec as P

ROW_EPS = 0.05
CHAN_EPS = 0.02
MESH = pl.DeviceIdType.MESH
CHUNKS = 8
CONV_CHUNKS = 4
LANES = 128
ROW_BLOCK = 32
CONV_BLOCK = 64
PAD = 32
SUBLANES = 8
FIRST_SLOT = 8
SECOND_SLOT = 2
THIRD_SLOT = 2
PER_SLOT = 2
UP, DOWN, OVER_X, OVER_Y = range(4)


def rms_rows(stream, gain_vec):
    square_mean = jnp.mean(stream * stream, axis=-1, keepdims=True)
    return (stream * lax.rsqrt(square_mean + ROW_EPS) * gain_vec.astype(jnp.float32)).astype(
        jnp.bfloat16
    )


def swap(value):
    size = lax.axis_size("tp")
    return lax.ppermute(value, "tp", [(i, size - 1 - i) for i in range(size)])


def widen(normed):
    return jnp.concatenate([normed, swap(normed)])


def narrow(partial_value):
    rounded = partial_value.astype(jnp.bfloat16)
    half = rounded.shape[0] // 2
    return rounded[:half].astype(jnp.float32) + swap(rounded[half:]).astype(jnp.float32)


def reorder(rows):
    half = rows.shape[0] // 2
    flipped = jnp.concatenate([rows[half:], rows[:half]])
    return jnp.where(lax.axis_index("tp") == 0, rows, flipped)


def place():
    fs = lax.axis_index("fs")
    return lax.axis_index("rep"), lax.rem(fs, 2), fs // 2


class Gather:
    def __init__(self, depth, ins, slots, local_sems, side_sems, send_sems, recv_sems):
        self.depth = depth
        self.ins, self.slots = ins, slots
        self.local_sems, self.recv_sems = local_sems, recv_sems
        self.side_sems, self.send_sems = side_sems, send_sems
        self.x, self.y, self.z = place()
        self.has_up, self.has_down = self.z + 1 < depth, self.z > 0
        self.own = self.z * 2 + self.y

    def target(self, way):
        if way == UP:
            return {"fs": (self.z + 1) * 2 + self.y}
        if way == DOWN:
            return {"fs": (self.z - 1) * 2 + self.y}
        if way == OVER_X:
            return {"rep": 1 - self.x}
        return {"fs": self.z * 2 + 1 - self.y}

    def barrier(self, *others):
        barrier = pltpu.get_barrier_semaphore()
        for target in (self.target(OVER_X), self.target(OVER_Y), *others):
            pl.semaphore_signal(barrier, inc=1, device_id=target, device_id_type=MESH)
        for way, present in ((UP, self.has_up), (DOWN, self.has_down)):

            @pl.when(present)
            def _(way=way):
                pl.semaphore_signal(barrier, inc=1, device_id=self.target(way), device_id_type=MESH)

        peers = 2 + len(others) + self.has_up.astype(jnp.int32) + self.has_down.astype(jnp.int32)
        pl.semaphore_wait(barrier, peers)

    def count(self, m):
        return self.slots[m].shape[0] // (2 * self.depth)

    def at_end(self, at):
        return jnp.logical_or(at == 0, at == self.depth - 1)

    def along(self, m, at):
        count = self.count(m)
        return jnp.where(self.at_end(at), count - count // 4, count)

    def across(self, m, d):
        count = self.count(m)
        far = jnp.clip(count // 2 + d - 1, count // 2, count - count // 4)
        return jnp.where(self.at_end(self.z), far, count // 2)

    def chunk(self, m, k, e):
        count = self.count(m)
        return k * count + e + self.x * (count - 1 - 2 * e)

    def locals(self, m):
        copies, first = [], 0
        for n, part in enumerate(self.ins[m]):
            height = part.shape[1]
            count = self.count(m)
            here = self.slots[m].at[pl.ds(self.own * count, count), pl.ds(first, height)]
            copies.append(pltpu.make_async_copy(part, here, self.local_sems.at[m, n]))
            first += height
        return copies

    def copy(self, m, c, way):
        piece = self.slots[m].at[c]
        recv_sem = self.side_sems.at[m] if way == OVER_X else self.recv_sems[m].at[c]
        return pltpu.make_async_remote_copy(
            src_ref=piece,
            dst_ref=piece,
            send_sem=self.send_sems.at[m, way],
            recv_sem=recv_sem,
            device_id=self.target(way),
            device_id_type=MESH,
        )

    def spread(self, m, k, e, ways):
        c = self.chunk(m, k, e)
        for way, wanted in ways:
            pl.when(wanted)(lambda way=way: self.copy(m, c, way).start())

    def start_local(self):
        for m in range(len(self.ins)):
            for part in self.locals(m):
                part.start()

    def start_own(self, m):
        for part in self.locals(m):
            part.wait()
        up, down = self.along(m, self.z + 1), self.along(m, self.z - 1)
        across = self.across(m, 0)

        def step(e, carry):
            self.spread(
                m,
                self.own,
                e,
                (
                    (UP, jnp.logical_and(self.has_up, e < up)),
                    (DOWN, jnp.logical_and(self.has_down, e < down)),
                    (OVER_Y, e < across),
                ),
            )
            return carry

        lax.fori_loop(0, self.count(m), step, 0)

    def pieces(self, d):
        below, above = self.z - d, self.z + d
        return (
            (below, below >= 0, self.z + 1, self.has_up, UP),
            (above, jnp.logical_and(d > 0, above < self.depth), self.z - 1, self.has_down, DOWN),
        )

    def arrive_along(self, m, d, e):
        along, across = self.along(m, self.z), self.across(m, d)
        spare = self.count(m) - along
        for at, present, goal, further, way in self.pieces(d):

            @pl.when(jnp.logical_and(present, e < along))
            def _(at=at, goal=goal, further=further, way=way):
                k = at * 2 + self.y
                self.copy(m, self.chunk(m, k, e), UP).wait_recv()
                onward = jnp.logical_and(further, e < self.along(m, goal))
                self.spread(m, k, e, ((way, onward), (OVER_Y, e < across), (OVER_X, e < spare)))

    def arrive_across(self, m, d, e):
        across = self.across(m, d)
        spare = self.count(m) - across
        for at, present, _, _, _ in self.pieces(d):

            @pl.when(jnp.logical_and(present, e < across))
            def _(at=at):
                k = at * 2 + 1 - self.y
                self.copy(m, self.chunk(m, k, e), OVER_Y).wait_recv()
                self.spread(m, k, e, ((OVER_X, e < spare),))

    def slots_of(self, m):
        return self.depth * self.count(m)

    def run(self, m, work=None):
        count = self.count(m)
        ahead = max(self.depth - 1, 0) * count

        def step(t, carry):
            r, e = lax.div(t, count), lax.rem(t, count)
            if m + 1 < len(self.ins):
                pl.when(t == ahead)(lambda: self.start_own(m + 1))
            self.arrive_along(m, r + 1, e)
            self.arrive_across(m, r, e)
            if work is not None:
                work(t)
            return carry

        lax.fori_loop(0, self.slots_of(m), step, 0)

    def totals(self, m, z):
        count, last = self.count(m), self.depth - 1
        least = count - count // 4

        def along(at):
            return least if at in (0, last) else count

        def across(d):
            return min(max(count // 2 + d - 1, count // 2), least) if z in (0, last) else count // 2

        distances = [0, *range(1, z + 1), *range(1, last - z + 1)]
        totals = [0] * 4
        if z < last:
            totals[UP] = along(z + 1) + z * min(along(z), along(z + 1))
        if z > 0:
            totals[DOWN] = along(z - 1) + (last - z) * min(along(z), along(z - 1))
        totals[OVER_Y] = sum(across(d) for d in distances)
        totals[OVER_X] = last * (count - along(z)) + sum(count - across(d) for d in distances)
        return totals

    def all_of(self, m, way, size):
        chunks = self.slots[m].at[pl.ds(0, size)]
        return pltpu.make_async_remote_copy(
            src_ref=chunks,
            dst_ref=chunks,
            send_sem=self.send_sems.at[m, way],
            recv_sem=self.side_sems.at[m],
            device_id=self.target(way),
            device_id_type=MESH,
        )

    def each_place(self, visit):
        for z in range(self.depth):
            pl.when(self.z == z)(lambda z=z: visit(z))

    def settle(self, m):
        self.each_place(lambda z: self.all_of(m, OVER_X, self.totals(m, z)[OVER_X]).wait_recv())

    def drain(self, m):
        def visit(z):
            for way, size in enumerate(self.totals(m, z)):
                if size:
                    self.all_of(m, way, size).wait_send()

        self.each_place(visit)


def gather_sems(total, parts, counts):
    dma = pltpu.SemaphoreType.DMA
    return [dma((len(counts), parts)), dma((len(counts),)), dma((len(counts), 4))] + [
        dma((total * count,)) for count in counts
    ]


def gather_kernel(depth, count, *refs):
    ins, slots = [(ref,) for ref in refs[:count]], refs[count : 2 * count]
    sems = refs[2 * count :]
    gather = Gather(depth, ins, slots, *sems[:3], sems[3:])
    gather.start_local()
    gather.barrier()
    gather.start_own(0)
    for m in range(count):
        gather.run(m)
    for m in range(count):
        gather.settle(m)
        gather.drain(m)


def gather_all(blocks):
    total = lax.axis_size("fs")
    count = len(blocks)
    outs = [jax.ShapeDtypeStruct((total * b.shape[0], *b.shape[1:]), b.dtype) for b in blocks]
    return pl.pallas_call(
        functools.partial(gather_kernel, total // 2, count),
        out_shape=outs,
        in_specs=[pl.BlockSpec(memory_space=pl.ANY)] * count,
        out_specs=[pl.BlockSpec(memory_space=pltpu.VMEM)] * count,
        scratch_shapes=gather_sems(total, 1, [b.shape[0] for b in blocks]),
        compiler_params=pltpu.CompilerParams(
            collective_id=0, has_side_effects=True, vmem_limit_bytes=48 * 2**20
        ),
        name="gather_all",
    )(*blocks)


def hidden_units(gathered, whole_gate, whole_up):
    gate_rows = jnp.dot(gathered, whole_gate, preferred_element_type=jnp.float32)
    up_rows = jnp.dot(gathered, whole_up, preferred_element_type=jnp.float32)
    return (jax.nn.silu(gate_rows) * up_rows).astype(jnp.bfloat16)


def columns_of(blocks):
    return blocks.transpose(1, 0, 2).reshape(blocks.shape[1], -1)


def causal_taps(glu, kernel):
    length = glu.shape[0]
    taps = kernel.shape[0]
    padded = jnp.pad(glu, ((taps - 1, 0), (0, 0)))
    output = jnp.zeros_like(glu)
    for tap_index in range(taps):
        output = output + padded[tap_index : tap_index + length] * kernel[tap_index]
    return output


def chunked(block, pieces):
    return block.reshape(pieces, block.shape[0] // pieces, block.shape[1])


class Layer:
    def __init__(self, gather, tokens, gains, taps, out, scratch):
        self.gather = gather
        self.out = out
        (
            self.own,
            self.stream,
            self.rows,
            self.hidden,
            self.partial,
            self.landed,
            self.padded,
            self.conv,
            self.sums,
            self.act,
            self.mixed,
            *self.packed,
            self.packed_taps,
            self.gains,
            self.gain,
            self.taps,
            self.own_sems,
            self.row_send,
            self.row_recv,
            self.part_send,
            self.part_recv,
            self.sum_send,
            self.sum_recv,
            self.out_sem,
        ) = scratch
        self.half, self.width = self.own.shape
        self.units = self.hidden.shape[1]
        self.total = gather.depth * 2
        self.piece = self.width // self.total
        self.blocks = self.half // ROW_BLOCK
        self.tp = lax.axis_index("tp")
        self.partner = {"tp": 1 - self.tp}
        self.mine = pl.multiple_of(self.tp * self.half, self.half)
        self.theirs = pl.multiple_of((1 - self.tp) * self.half, self.half)
        inputs = (tokens, *gains, taps)
        self.loads = [
            pltpu.make_async_copy(src, dst, self.own_sems.at[n])
            for n, (src, dst) in enumerate(zip(inputs, (self.own, *self.packed, self.packed_taps)))
        ]

    def expand(self):
        for n, packed in enumerate(self.packed):
            target = self.gain if n == 3 else self.gains.at[n]
            for j in range(packed.shape[0]):
                row = packed[j : j + 1, :].astype(jnp.float32)
                target[:, j * LANES : (j + 1) * LANES] = jnp.broadcast_to(row, (SUBLANES, LANES))
        for j in range(self.taps.shape[0]):
            row = self.packed_taps[j : j + 1, :].astype(jnp.float32)
            self.taps[j] = jnp.broadcast_to(row, (SUBLANES, row.shape[1]))

    def remote(self, src, dst, send_sem, recv_sem):
        return pltpu.make_async_remote_copy(
            src_ref=src,
            dst_ref=dst,
            send_sem=send_sem,
            recv_sem=recv_sem,
            device_id=self.partner,
            device_id_type=MESH,
        )

    def row_copy(self, n, first, count):
        here = self.rows.at[n, pl.ds(first, count)]
        return self.remote(here, here, self.row_send.at[n], self.row_recv.at[n])

    def await_rows(self, n):
        self.row_copy(n, self.theirs, self.half).wait_recv()

    def part_copy(self, n, k, width=None):
        cols = pl.ds(pl.multiple_of(k * self.piece, self.piece), self.piece if width is None else width)
        return self.remote(
            self.partial.at[n, pl.ds(self.theirs, self.half), cols],
            self.landed.at[n, :, cols],
            self.part_send.at[n],
            self.part_recv.at[n + (k if n == 2 else 0)],
        )

    def sum_copy(self):
        return self.remote(self.sums.at[0], self.sums.at[1], self.sum_send.at[0], self.sum_recv.at[0])

    def norm(self, n, i, stream):
        square_mean = jnp.mean(stream * stream, axis=-1, keepdims=True)
        scaled = (stream * lax.rsqrt(square_mean + ROW_EPS)).reshape(-1, SUBLANES, self.width) * self.gains[n][None]
        rows = pl.ds(self.mine + self.block(i), ROW_BLOCK)
        self.rows[n, rows, :] = scaled.reshape(stream.shape).astype(jnp.bfloat16)
        self.row_copy(n, self.mine + self.block(i), ROW_BLOCK).start()

    def block(self, i):
        return pl.multiple_of(i * ROW_BLOCK, ROW_BLOCK)

    def start_rows(self):
        def step(i, carry):
            self.norm(0, i, self.own[pl.ds(self.block(i), ROW_BLOCK), :].astype(jnp.float32))
            return carry

        lax.fori_loop(0, self.blocks, step, 0)

    def update(self, n, i, scale):
        first = self.block(i)
        here = pl.ds(first, ROW_BLOCK)
        before = self.own[here, :].astype(jnp.float32) if n == 0 else self.stream[here, :]
        added = self.partial[n, pl.ds(self.mine + first, ROW_BLOCK), :].astype(jnp.float32) + self.landed[
            n, here, :
        ].astype(jnp.float32)
        stream = before + (added if scale is None else scale * added)
        self.stream[here, :] = stream
        self.norm(n + 1, i, stream)

    def await_parts(self, n):
        self.part_copy(n, 0, self.width).wait_recv()

    def matrix(self, m, first, size):
        return self.gather.slots[m][:, :, pl.ds(first, size)].reshape(self.width, size)

    def columns(self, m, k):
        count = self.gather.count(m)
        return self.gather.slots[m][pl.ds(k * count, count)].reshape(-1, self.piece)

    def hidden_tile(self, n, row, height, first, size):
        rows = self.rows[n, pl.ds(row, height), :]
        gate = jnp.dot(rows, self.matrix(0, first, size), preferred_element_type=jnp.float32)
        up = jnp.dot(rows, self.matrix(1, first, size), preferred_element_type=jnp.float32)
        self.hidden[pl.ds(row, height), pl.ds(first, size)] = (jax.nn.silu(gate) * up).astype(jnp.bfloat16)

    def down_piece(self, n, k):
        weights = self.columns(2, k)
        result = jnp.dot(self.hidden[...], weights, preferred_element_type=jnp.float32)
        cols = pl.ds(pl.multiple_of(k * self.piece, self.piece), self.piece)
        self.partial[n, :, cols] = result.astype(jnp.bfloat16)
        self.part_copy(n, k).start()

    def first_work(self, t):
        j = t - FIRST_SLOT

        @pl.when(j == 0)
        def _():
            self.gather.settle(0)
            self.gather.settle(1)
            self.await_rows(0)

        @pl.when(jnp.logical_and(j >= 0, j < self.units // LANES))
        def _():
            self.hidden_tile(0, 0, 2 * self.half, pl.multiple_of(j * LANES, LANES), LANES)

    def second_work(self, t):
        pl.when(t == SECOND_SLOT)(lambda: self.gather.settle(2))

        def step(u, carry):
            j = (t - SECOND_SLOT) * PER_SLOT + u
            i = j - self.total
            pl.when(jnp.logical_and(j >= 0, i < 0))(lambda: self.down_piece(0, j))
            pl.when(i == 0)(lambda: self.await_parts(0))
            pl.when(jnp.logical_and(i >= 0, i < self.blocks))(lambda: self.update(0, i, 0.5))
            return carry

        lax.fori_loop(0, PER_SLOT, step, 0)

    def third_work(self, t):
        blocks = 2 * self.half // CONV_BLOCK

        def step(u, carry):
            j = (t - THIRD_SLOT) * PER_SLOT + u
            i = j - 2

            @pl.when(jnp.logical_or(j == 0, j == 1))
            def _():
                pl.when(j == 0)(lambda: self.gather.settle(3))
                pl.when(j == 1)(lambda: self.await_rows(1))
                self.gated(pl.multiple_of(jnp.where(j == 0, self.mine, self.theirs), self.half))

            pl.when(jnp.logical_and(i >= 0, i < blocks))(lambda: self.convolve(i))
            pl.when(i == blocks)(lambda: self.sum_copy().start())
            return carry

        lax.fori_loop(0, PER_SLOT, step, 0)

    def gated(self, row):
        rows = self.rows[1, pl.ds(row, self.half), :]
        whole = self.gather.slots[3]
        height = whole.shape[1] // 2
        value = whole[:, :height, :].reshape(self.width, -1)
        gate = whole[:, height:, :].reshape(self.width, -1)
        values = jnp.dot(rows, value, preferred_element_type=jnp.float32)
        gates = jnp.dot(rows, gate, preferred_element_type=jnp.float32)
        self.padded[pl.ds(PAD + row, self.half), :] = values * jax.nn.sigmoid(gates)

    def convolve(self, i):
        taps = self.taps.shape[0]
        lanes = self.sums.shape[-1]
        first = pl.multiple_of(i * CONV_BLOCK, CONV_BLOCK)
        window = self.padded[pl.ds(first, CONV_BLOCK + PAD), :]
        channels = window.shape[1]
        total = jnp.zeros((CONV_BLOCK // SUBLANES, SUBLANES, channels), jnp.float32)
        offsets = [PAD - (taps - 1) + j for j in range(taps)]
        for shift in range(SUBLANES):
            mine = [(j, at) for j, at in enumerate(offsets) if at % SUBLANES == shift]
            reach = max(at for _, at in mine) - shift + CONV_BLOCK
            shifted = window[shift : shift + reach]
            for j, at in mine:
                block = shifted[at - shift : at - shift + CONV_BLOCK].reshape(total.shape)
                total = total + block * self.taps[j][None]
        total = total.reshape(CONV_BLOCK, channels)
        here = pl.ds(first, CONV_BLOCK)
        self.conv[here, :] = total
        plain = jnp.sum(total, axis=-1, keepdims=True)
        squared = jnp.sum(total * total, axis=-1, keepdims=True)
        lane = lax.broadcasted_iota(jnp.int32, (CONV_BLOCK, lanes), 1)
        self.sums[0, here, :] = jnp.where(lane < lanes // 2, plain, squared)

    def activate(self):
        lanes = self.sums.shape[-1]
        channels = 2 * self.conv.shape[1]

        def step(i, carry):
            here = pl.ds(pl.multiple_of(i * CONV_BLOCK, CONV_BLOCK), CONV_BLOCK)
            sums = (self.sums[0, here, :] + self.sums[1, here, :]) / channels
            average, square = sums[:, :1], sums[:, lanes // 2 : lanes // 2 + 1]
            spread = jnp.maximum(square - average * average, 0.0)
            scaled = (self.conv[here, :] - average) * lax.rsqrt(spread + CHAN_EPS)
            scaled = scaled.reshape(-1, SUBLANES, scaled.shape[1]) * self.gain[...][None]
            self.act[here, :] = jax.nn.silu(scaled.reshape(CONV_BLOCK, -1)).astype(jnp.bfloat16)
            return carry

        lax.fori_loop(0, 2 * self.half // CONV_BLOCK, step, 0)

    def mix(self):
        def step(k, carry):
            weights = self.columns(4, k)
            result = jnp.dot(self.act[...], weights, preferred_element_type=jnp.float32)
            cols = pl.ds(pl.multiple_of(k * self.piece, self.piece), self.piece)
            self.partial[1, :, cols] = result.astype(jnp.bfloat16)
            self.part_copy(1, k).start()
            return carry

        lax.fori_loop(0, self.total, step, 0)

    def finish_conv(self):
        self.sum_copy().wait_recv()
        self.activate()
        self.gather.settle(4)
        self.mix()
        self.await_parts(1)

        def step(i, carry):
            self.update(1, i, None)
            return carry

        lax.fori_loop(0, self.blocks, step, 0)

    def second_half_step(self):
        tile = 2 * LANES
        whole = self.units // tile
        early = min(2, whole)

        def split(i, carry):
            pl.when(i == early)(lambda: self.await_rows(2))
            row = jnp.where(i < early, self.mine, self.theirs)
            first = pl.multiple_of(lax.rem(i, early) * tile, tile)
            self.hidden_tile(2, pl.multiple_of(row, self.half), self.half, first, tile)
            return carry

        lax.fori_loop(0, 2 * early, split, 0)

        def step(j, carry):
            self.hidden_tile(2, 0, 2 * self.half, pl.multiple_of(j * tile, tile), tile)
            return carry

        lax.fori_loop(early, whole, step, 0)
        if self.units % tile:
            self.hidden_tile(2, 0, 2 * self.half, whole * tile, self.units % tile)

        def piece(k, carry):
            self.down_piece(2, k)
            return carry

        lax.fori_loop(0, self.total, piece, 0)

        def finish(k, carry):
            self.part_copy(2, k).wait_recv()
            cols = pl.ds(pl.multiple_of(k * self.piece, self.piece), self.piece)
            added = self.partial[2, pl.ds(self.mine, self.half), cols].astype(jnp.float32) + self.landed[
                2, :, cols
            ].astype(jnp.float32)
            self.mixed[:, cols] = (self.stream[:, cols] + 0.5 * added).astype(self.mixed.dtype)
            pltpu.make_async_copy(self.mixed.at[:, cols], self.out.at[:, cols], self.out_sem.at[0]).start()
            return carry

        lax.fori_loop(0, self.total, finish, 0)

    def drain(self):
        self.sum_copy().wait_send()
        for n in range(3):
            self.row_copy(n, self.mine, self.half).wait_send()
            self.part_copy(n, 0, self.width).wait_send()

    def run(self):
        gather = self.gather
        gather.start_local()
        for load in self.loads:
            load.start()
        gather.barrier(self.partner)
        gather.start_own(0)
        for load in self.loads:
            load.wait()
        self.expand()
        self.start_rows()
        self.padded[:PAD, :] = jnp.zeros((PAD, self.padded.shape[1]), jnp.float32)
        gather.run(0)
        gather.run(1)
        gather.run(2, self.first_work)
        gather.run(3, self.second_work)
        gather.run(4, self.third_work)
        self.finish_conv()
        self.second_half_step()
        for m in range(len(gather.ins)):
            gather.drain(m)
        self.drain()
        pltpu.make_async_copy(self.mixed, self.out, self.out_sem.at[0]).wait()


def layer_kernel(depth, *refs):
    tokens, gains, taps, refs = refs[0], refs[1:5], refs[5], refs[6:]
    ins, refs = ((refs[0],), (refs[1],), (refs[2],), refs[3:5], (refs[5],)), refs[6:]
    out, refs = refs[0], refs[1:]
    slots, sems, scratch = refs[:5], refs[5:13], refs[13:]
    gather = Gather(depth, ins, slots, *sems[:3], sems[3:])
    Layer(gather, tokens, gains, taps, out, scratch).run()


def fused_layer(tokens, gains, depthwise, blocks, smalls):
    total = lax.axis_size("fs")
    half, width = tokens.shape
    units, (taps, channels) = blocks[0].shape[2], depthwise.shape
    vmem, dma = pltpu.VMEM, pltpu.SemaphoreType.DMA
    count, height, piece = smalls[0].shape
    shapes = [b.shape for b in blocks] + [(count, 2 * height, piece), (count, height, piece)]
    f32, bf16 = jnp.float32, jnp.bfloat16
    return pl.pallas_call(
        functools.partial(layer_kernel, total // 2),
        out_shape=jax.ShapeDtypeStruct((half, width), bf16),
        in_specs=[pl.BlockSpec(memory_space=pltpu.HBM)] * 12,
        out_specs=pl.BlockSpec(memory_space=pltpu.HBM),
        scratch_shapes=[vmem((total * shape[0], *shape[1:]), bf16) for shape in shapes]
        + gather_sems(total, 2, [shape[0] for shape in shapes])
        + [
            vmem((half, width), bf16),
            vmem((half, width), f32),
            vmem((3, 2 * half, width), bf16),
            vmem((2 * half, units), bf16),
            vmem((3, 2 * half, width), bf16),
            vmem((3, half, width), bf16),
            vmem((PAD + 2 * half, channels), f32),
            vmem((2 * half, channels), f32),
            vmem((2, 2 * half, LANES), f32),
            vmem((2 * half, channels), bf16),
            vmem((half, width), bf16),
        ]
        + [vmem(gain.shape, bf16) for gain in gains]
        + [
            vmem(depthwise.shape, bf16),
            vmem((3, SUBLANES, width), f32),
            vmem((SUBLANES, channels), f32),
            vmem((taps, SUBLANES, channels), f32),
            dma((6,)),
            dma((3,)),
            dma((3,)),
            dma((3,)),
            dma((2 + total,)),
            dma((1,)),
            dma((1,)),
            dma((1,)),
        ],
        compiler_params=pltpu.CompilerParams(
            collective_id=0, has_side_effects=True, vmem_limit_bytes=58 * 2**20
        ),
        name="fused_layer",
    )(tokens, *gains, depthwise, *blocks, *smalls)


def fits(half, ffn_gate, ffn_down, conv_value, conv_out, depthwise):
    piece, total = ffn_gate.shape[0], lax.axis_size("fs")
    slots, conv_slots = total // 2 * CHUNKS, total // 2 * CONV_CHUNKS
    return (
        piece % (16 * CHUNKS) == 0
        and ffn_down.shape[0] % (16 * CHUNKS) == 0
        and conv_out.shape[0] == piece
        and conv_value.shape[1] == piece
        and piece % LANES == 0
        and ffn_gate.shape[1] % LANES == 0
        and half % ROW_BLOCK == 0
        and half % CONV_BLOCK == 0
        and depthwise.shape[0] <= PAD
        and slots >= FIRST_SLOT + ffn_gate.shape[1] // LANES
        and (conv_slots - SECOND_SLOT) * PER_SLOT >= total + half // ROW_BLOCK
        and (conv_slots - THIRD_SLOT) * PER_SLOT > 2 + 2 * half // CONV_BLOCK
        and lax.axis_size("tp") == 2
        and lax.axis_size("rep") == 2
    )


def shards(
    tokens,
    norm_first,
    norm_mixer,
    norm_second,
    ffn_gate,
    ffn_up,
    ffn_down,
    conv_value,
    conv_gate,
    depthwise,
    conv_gain,
    conv_out,
):
    width = tokens.shape[-1]
    if fits(tokens.size // width, ffn_gate, ffn_down, conv_value, conv_out, depthwise):
        mixed = fused_layer(
            tokens.reshape(-1, width),
            [gain.reshape(-1, LANES) for gain in (norm_first, norm_mixer, norm_second, conv_gain)],
            depthwise,
            [chunked(block, CHUNKS) for block in (ffn_gate, ffn_up, ffn_down)],
            [chunked(block, CONV_CHUNKS) for block in (conv_value, conv_gate, conv_out)],
        )
        return mixed.reshape(tokens.shape)
    stream = tokens.reshape(-1, width).astype(jnp.float32)
    first_rows = widen(rms_rows(stream, norm_first))
    small = jnp.concatenate([conv_value, conv_gate, conv_out.reshape(-1, conv_value.shape[1])])
    gate, up, down, small_all = gather_all(
        [chunked(block, CHUNKS) for block in (ffn_gate, ffn_up, ffn_down, small)]
    )
    whole_gate = gate.reshape(-1, gate.shape[-1])
    whole_up = up.reshape(-1, up.shape[-1])
    total = lax.axis_size("fs")
    whole_down = columns_of(down.reshape(total, -1, down.shape[-1]))
    small_all = small_all.reshape(total, -1, small_all.shape[-1])
    rows = conv_value.shape[0]
    channels_here = conv_value.shape[1]
    whole_value = small_all[:, :rows].reshape(-1, channels_here)
    whole_conv_gate = small_all[:, rows : 2 * rows].reshape(-1, channels_here)
    whole_out = columns_of(small_all[:, 2 * rows :].reshape(total, *conv_out.shape))

    hidden = hidden_units(first_rows, whole_gate, whole_up)
    stream = stream + 0.5 * narrow(jnp.dot(hidden, whole_down, preferred_element_type=jnp.float32))
    gathered = widen(rms_rows(stream, norm_mixer))
    values = jnp.dot(gathered, whole_value, preferred_element_type=jnp.float32)
    gates = jnp.dot(gathered, whole_conv_gate, preferred_element_type=jnp.float32)
    glu = reorder(values * jax.nn.sigmoid(gates))
    conv = causal_taps(glu, depthwise.astype(jnp.float32))
    channels = conv.shape[1] * lax.axis_size("tp")
    sums, squares = lax.psum((jnp.sum(conv, axis=1), jnp.sum(conv * conv, axis=1)), "tp")
    average = sums / channels
    spread = jnp.maximum(squares / channels - average * average, 0.0)
    centred = conv - average[:, None]
    activated = jax.nn.silu(
        centred * lax.rsqrt(spread[:, None] + CHAN_EPS) * conv_gain.astype(jnp.float32)
    ).astype(jnp.bfloat16)
    stream = stream + narrow(jnp.dot(reorder(activated), whole_out, preferred_element_type=jnp.float32))
    second_rows = widen(rms_rows(stream, norm_second))
    second_hidden = hidden_units(second_rows, whole_gate, whole_up)
    stream = stream + 0.5 * narrow(jnp.dot(second_hidden, whole_down, preferred_element_type=jnp.float32))
    return stream.astype(jnp.bfloat16).reshape(tokens.shape)


def solution(mesh):
    in_specs = (
        P(("rep", "fs"), "tp", None),
        P(),
        P(),
        P(),
        P("fs", "tp"),
        P("fs", "tp"),
        P("tp", "fs"),
        P("fs", "tp"),
        P("fs", "tp"),
        P(None, "tp"),
        P("tp"),
        P("tp", "fs"),
    )
    out_specs = P(("rep", "fs"), "tp", None)
    return jax.shard_map(shards, mesh=mesh, in_specs=in_specs, out_specs=out_specs, check_vma=False)
```

```python
import functools

import jax
import jax.numpy as jnp
from jax import lax
from jax.experimental import pallas as pl
from jax.experimental.pallas import tpu as pltpu
from jax.sharding import PartitionSpec as P

ROW_EPS = 0.05
CHAN_EPS = 0.02
MESH = pl.DeviceIdType.MESH
CHUNKS = 8
CONV_CHUNKS = 4
LANES = 128
ROW_BLOCK = 32
CONV_BLOCK = 64
PAD = 32
SUBLANES = 8
FIRST_SLOT = 8
SECOND_SLOT = 2
THIRD_SLOT = 2
PER_SLOT = 2
SUM_WAIT = 4
MIX_GROUP = 4
DOWN_GROUP = 2
UP, DOWN, OVER_X, OVER_Y = range(4)


def rms_rows(stream, gain_vec):
    square_mean = jnp.mean(stream * stream, axis=-1, keepdims=True)
    return (stream * lax.rsqrt(square_mean + ROW_EPS) * gain_vec.astype(jnp.float32)).astype(
        jnp.bfloat16
    )


def swap(value):
    size = lax.axis_size("tp")
    return lax.ppermute(value, "tp", [(i, size - 1 - i) for i in range(size)])


def widen(normed):
    return jnp.concatenate([normed, swap(normed)])


def narrow(partial_value):
    rounded = partial_value.astype(jnp.bfloat16)
    half = rounded.shape[0] // 2
    return rounded[:half].astype(jnp.float32) + swap(rounded[half:]).astype(jnp.float32)


def reorder(rows):
    half = rows.shape[0] // 2
    flipped = jnp.concatenate([rows[half:], rows[:half]])
    return jnp.where(lax.axis_index("tp") == 0, rows, flipped)


def place():
    fs = lax.axis_index("fs")
    return lax.axis_index("rep"), lax.rem(fs, 2), fs // 2


class Gather:
    def __init__(self, depth, ins, slots, local_sems, side_sems, send_sems, recv_sems):
        self.depth = depth
        self.ins, self.slots = ins, slots
        self.local_sems, self.recv_sems = local_sems, recv_sems
        self.side_sems, self.send_sems = side_sems, send_sems
        self.x, self.y, self.z = place()
        self.has_up, self.has_down = self.z + 1 < depth, self.z > 0
        self.own = self.z * 2 + self.y

    def target(self, way):
        if way == UP:
            return {"fs": (self.z + 1) * 2 + self.y}
        if way == DOWN:
            return {"fs": (self.z - 1) * 2 + self.y}
        if way == OVER_X:
            return {"rep": 1 - self.x}
        return {"fs": self.z * 2 + 1 - self.y}

    def barrier(self, *others):
        barrier = pltpu.get_barrier_semaphore()
        for target in (self.target(OVER_X), self.target(OVER_Y), *others):
            pl.semaphore_signal(barrier, inc=1, device_id=target, device_id_type=MESH)
        for way, present in ((UP, self.has_up), (DOWN, self.has_down)):

            @pl.when(present)
            def _(way=way):
                pl.semaphore_signal(barrier, inc=1, device_id=self.target(way), device_id_type=MESH)

        peers = 2 + len(others) + self.has_up.astype(jnp.int32) + self.has_down.astype(jnp.int32)
        pl.semaphore_wait(barrier, peers)

    def count(self, m):
        return self.slots[m].shape[0] // (2 * self.depth)

    def at_end(self, at):
        return jnp.logical_or(at == 0, at == self.depth - 1)

    def along(self, m, at):
        count = self.count(m)
        return jnp.where(self.at_end(at), count - count // 4, count)

    def across(self, m, d):
        count = self.count(m)
        far = jnp.clip(count // 2 + d - 1, count // 2, count - count // 4)
        return jnp.where(self.at_end(self.z), far, count // 2)

    def chunk(self, m, k, e):
        count = self.count(m)
        return k * count + e + self.x * (count - 1 - 2 * e)

    def locals(self, m):
        copies, first = [], 0
        for n, part in enumerate(self.ins[m]):
            height = part.shape[1]
            count = self.count(m)
            here = self.slots[m].at[pl.ds(self.own * count, count), pl.ds(first, height)]
            copies.append(pltpu.make_async_copy(part, here, self.local_sems.at[m, n]))
            first += height
        return copies

    def copy(self, m, c, way):
        piece = self.slots[m].at[c]
        recv_sem = self.side_sems.at[m] if way == OVER_X else self.recv_sems[m].at[c]
        return pltpu.make_async_remote_copy(
            src_ref=piece,
            dst_ref=piece,
            send_sem=self.send_sems.at[m, way],
            recv_sem=recv_sem,
            device_id=self.target(way),
            device_id_type=MESH,
        )

    def spread(self, m, k, e, ways):
        c = self.chunk(m, k, e)
        for way, wanted in ways:
            pl.when(wanted)(lambda way=way: self.copy(m, c, way).start())

    def start_local(self):
        for m in range(len(self.ins)):
            for part in self.locals(m):
                part.start()

    def start_own(self, m):
        for part in self.locals(m):
            part.wait()
        up, down = self.along(m, self.z + 1), self.along(m, self.z - 1)
        across = self.across(m, 0)

        def step(e, carry):
            self.spread(
                m,
                self.own,
                e,
                (
                    (UP, jnp.logical_and(self.has_up, e < up)),
                    (DOWN, jnp.logical_and(self.has_down, e < down)),
                    (OVER_Y, e < across),
                ),
            )
            return carry

        lax.fori_loop(0, self.count(m), step, 0)

    def pieces(self, d):
        below, above = self.z - d, self.z + d
        return (
            (below, below >= 0, self.z + 1, self.has_up, UP),
            (above, jnp.logical_and(d > 0, above < self.depth), self.z - 1, self.has_down, DOWN),
        )

    def arrive_along(self, m, d, e):
        along, across = self.along(m, self.z), self.across(m, d)
        spare = self.count(m) - along
        for at, present, goal, further, way in self.pieces(d):

            @pl.when(jnp.logical_and(present, e < along))
            def _(at=at, goal=goal, further=further, way=way):
                k = at * 2 + self.y
                self.copy(m, self.chunk(m, k, e), UP).wait_recv()
                onward = jnp.logical_and(further, e < self.along(m, goal))
                self.spread(m, k, e, ((way, onward), (OVER_Y, e < across), (OVER_X, e < spare)))

    def arrive_across(self, m, d, e):
        across = self.across(m, d)
        spare = self.count(m) - across
        for at, present, _, _, _ in self.pieces(d):

            @pl.when(jnp.logical_and(present, e < across))
            def _(at=at):
                k = at * 2 + 1 - self.y
                self.copy(m, self.chunk(m, k, e), OVER_Y).wait_recv()
                self.spread(m, k, e, ((OVER_X, e < spare),))

    def slots_of(self, m):
        return self.depth * self.count(m)

    def run(self, m, work=None):
        count = self.count(m)
        ahead = max(self.depth - 1, 0) * count

        def step(t, carry):
            r, e = lax.div(t, count), lax.rem(t, count)
            if m + 1 < len(self.ins):
                pl.when(t == ahead)(lambda: self.start_own(m + 1))
            self.arrive_along(m, r + 1, e)
            self.arrive_across(m, r, e)
            if work is not None:
                work(t)
            return carry

        lax.fori_loop(0, self.slots_of(m), step, 0)

    def totals(self, m, z):
        count, last = self.count(m), self.depth - 1
        least = count - count // 4

        def along(at):
            return least if at in (0, last) else count

        def across(d):
            return min(max(count // 2 + d - 1, count // 2), least) if z in (0, last) else count // 2

        distances = [0, *range(1, z + 1), *range(1, last - z + 1)]
        totals = [0] * 4
        if z < last:
            totals[UP] = along(z + 1) + z * min(along(z), along(z + 1))
        if z > 0:
            totals[DOWN] = along(z - 1) + (last - z) * min(along(z), along(z - 1))
        totals[OVER_Y] = sum(across(d) for d in distances)
        totals[OVER_X] = last * (count - along(z)) + sum(count - across(d) for d in distances)
        return totals

    def all_of(self, m, way, size):
        chunks = self.slots[m].at[pl.ds(0, size)]
        return pltpu.make_async_remote_copy(
            src_ref=chunks,
            dst_ref=chunks,
            send_sem=self.send_sems.at[m, way],
            recv_sem=self.side_sems.at[m],
            device_id=self.target(way),
            device_id_type=MESH,
        )

    def each_place(self, visit):
        for z in range(self.depth):
            pl.when(self.z == z)(lambda z=z: visit(z))

    def settle(self, m):
        self.each_place(lambda z: self.all_of(m, OVER_X, self.totals(m, z)[OVER_X]).wait_recv())

    def drain(self, m):
        def visit(z):
            for way, size in enumerate(self.totals(m, z)):
                if size:
                    self.all_of(m, way, size).wait_send()

        self.each_place(visit)


def gather_sems(total, parts, counts):
    dma = pltpu.SemaphoreType.DMA
    return [dma((len(counts), parts)), dma((len(counts),)), dma((len(counts), 4))] + [
        dma((total * count,)) for count in counts
    ]


def gather_kernel(depth, count, *refs):
    ins, slots = [(ref,) for ref in refs[:count]], refs[count : 2 * count]
    sems = refs[2 * count :]
    gather = Gather(depth, ins, slots, *sems[:3], sems[3:])
    gather.start_local()
    gather.barrier()
    gather.start_own(0)
    for m in range(count):
        gather.run(m)
    for m in range(count):
        gather.settle(m)
        gather.drain(m)


def gather_all(blocks):
    total = lax.axis_size("fs")
    count = len(blocks)
    outs = [jax.ShapeDtypeStruct((total * b.shape[0], *b.shape[1:]), b.dtype) for b in blocks]
    return pl.pallas_call(
        functools.partial(gather_kernel, total // 2, count),
        out_shape=outs,
        in_specs=[pl.BlockSpec(memory_space=pl.ANY)] * count,
        out_specs=[pl.BlockSpec(memory_space=pltpu.VMEM)] * count,
        scratch_shapes=gather_sems(total, 1, [b.shape[0] for b in blocks]),
        compiler_params=pltpu.CompilerParams(
            collective_id=0, has_side_effects=True, vmem_limit_bytes=48 * 2**20
        ),
        name="gather_all",
    )(*blocks)


def hidden_units(gathered, whole_gate, whole_up):
    gate_rows = jnp.dot(gathered, whole_gate, preferred_element_type=jnp.float32)
    up_rows = jnp.dot(gathered, whole_up, preferred_element_type=jnp.float32)
    return (jax.nn.silu(gate_rows) * up_rows).astype(jnp.bfloat16)


def columns_of(blocks):
    return blocks.transpose(1, 0, 2).reshape(blocks.shape[1], -1)


def causal_taps(glu, kernel):
    length = glu.shape[0]
    taps = kernel.shape[0]
    padded = jnp.pad(glu, ((taps - 1, 0), (0, 0)))
    output = jnp.zeros_like(glu)
    for tap_index in range(taps):
        output = output + padded[tap_index : tap_index + length] * kernel[tap_index]
    return output


def chunked(block, pieces):
    return block.reshape(pieces, block.shape[0] // pieces, block.shape[1])


class Layer:
    def __init__(self, gather, tokens, gains, taps, out, scratch):
        self.gather = gather
        self.out = out
        (
            self.own,
            self.stream,
            self.rows,
            self.hidden,
            self.partial,
            self.landed,
            self.padded,
            self.conv,
            self.sums,
            self.act,
            self.mixed,
            *self.packed,
            self.packed_taps,
            self.gains,
            self.gain,
            self.taps,
            self.own_sems,
            self.row_send,
            self.row_recv,
            self.part_send,
            self.part_recv,
            self.sum_send,
            self.sum_recv,
            self.out_sem,
        ) = scratch
        self.half, self.width = self.own.shape
        self.units = self.hidden.shape[1]
        self.total = gather.depth * 2
        self.piece = self.width // self.total
        self.blocks = self.half // ROW_BLOCK
        self.tp = lax.axis_index("tp")
        self.partner = {"tp": 1 - self.tp}
        self.mine = pl.multiple_of(self.tp * self.half, self.half)
        self.theirs = pl.multiple_of((1 - self.tp) * self.half, self.half)
        inputs = (tokens, *gains, taps)
        self.loads = [
            pltpu.make_async_copy(src, dst, self.own_sems.at[n])
            for n, (src, dst) in enumerate(zip(inputs, (self.own, *self.packed, self.packed_taps)))
        ]

    def expand(self):
        for n, packed in enumerate(self.packed):
            target = self.gain if n == 3 else self.gains.at[n]
            for j in range(packed.shape[0]):
                row = packed[j : j + 1, :].astype(jnp.float32)
                target[:, j * LANES : (j + 1) * LANES] = jnp.broadcast_to(row, (SUBLANES, LANES))
        for j in range(self.taps.shape[0]):
            row = self.packed_taps[j : j + 1, :].astype(jnp.float32)
            self.taps[j] = jnp.broadcast_to(row, (SUBLANES, row.shape[1]))

    def remote(self, src, dst, send_sem, recv_sem):
        return pltpu.make_async_remote_copy(
            src_ref=src,
            dst_ref=dst,
            send_sem=send_sem,
            recv_sem=recv_sem,
            device_id=self.partner,
            device_id_type=MESH,
        )

    def row_copy(self, n, first, count):
        here = self.rows.at[n, pl.ds(first, count)]
        return self.remote(here, here, self.row_send.at[n], self.row_recv.at[n])

    def await_rows(self, n):
        self.row_copy(n, self.theirs, self.half).wait_recv()

    def part_copy(self, n, k, width=None):
        cols = pl.ds(pl.multiple_of(k * self.piece, self.piece), self.piece if width is None else width)
        return self.remote(
            self.partial.at[n, pl.ds(self.theirs, self.half), cols],
            self.landed.at[n, :, cols],
            self.part_send.at[n],
            self.part_recv.at[n + (k if n == 2 else 0)],
        )

    def sum_copy(self):
        return self.remote(self.sums.at[0], self.sums.at[1], self.sum_send.at[0], self.sum_recv.at[0])

    def norm(self, n, i, stream):
        square_mean = jnp.mean(stream * stream, axis=-1, keepdims=True)
        scaled = (stream * lax.rsqrt(square_mean + ROW_EPS)).reshape(-1, SUBLANES, self.width) * self.gains[n][None]
        rows = pl.ds(self.mine + self.block(i), ROW_BLOCK)
        self.rows[n, rows, :] = scaled.reshape(stream.shape).astype(jnp.bfloat16)
        self.row_copy(n, self.mine + self.block(i), ROW_BLOCK).start()

    def block(self, i):
        return pl.multiple_of(i * ROW_BLOCK, ROW_BLOCK)

    def start_rows(self):
        def step(i, carry):
            self.norm(0, i, self.own[pl.ds(self.block(i), ROW_BLOCK), :].astype(jnp.float32))
            return carry

        lax.fori_loop(0, self.blocks, step, 0)

    def update(self, n, i, scale):
        first = self.block(i)
        here = pl.ds(first, ROW_BLOCK)
        before = self.own[here, :].astype(jnp.float32) if n == 0 else self.stream[here, :]
        added = self.partial[n, pl.ds(self.mine + first, ROW_BLOCK), :].astype(jnp.float32) + self.landed[
            n, here, :
        ].astype(jnp.float32)
        stream = before + (added if scale is None else scale * added)
        self.stream[here, :] = stream
        self.norm(n + 1, i, stream)

    def await_parts(self, n):
        self.part_copy(n, 0, self.width).wait_recv()

    def matrix(self, m, first, size):
        return self.gather.slots[m][:, :, pl.ds(first, size)].reshape(self.width, size)

    def columns(self, m, k):
        count = self.gather.count(m)
        return self.gather.slots[m][pl.ds(k * count, count)].reshape(-1, self.piece)

    def hidden_tile(self, n, row, height, first, size):
        rows = self.rows[n, pl.ds(row, height), :]
        gate = jnp.dot(rows, self.matrix(0, first, size), preferred_element_type=jnp.float32)
        up = jnp.dot(rows, self.matrix(1, first, size), preferred_element_type=jnp.float32)
        self.hidden[pl.ds(row, height), pl.ds(first, size)] = (jax.nn.silu(gate) * up).astype(jnp.bfloat16)

    def down_piece(self, n, k):
        weights = self.columns(2, k)
        result = jnp.dot(self.hidden[...], weights, preferred_element_type=jnp.float32)
        cols = pl.ds(pl.multiple_of(k * self.piece, self.piece), self.piece)
        self.partial[n, :, cols] = result.astype(jnp.bfloat16)
        self.part_copy(n, k).start()

    def first_work(self, t):
        j = t - FIRST_SLOT

        @pl.when(j == 0)
        def _():
            self.gather.settle(0)
            self.gather.settle(1)
            self.await_rows(0)

        @pl.when(jnp.logical_and(j >= 0, j < self.units // LANES))
        def _():
            self.hidden_tile(0, 0, 2 * self.half, pl.multiple_of(j * LANES, LANES), LANES)

    def second_work(self, t):
        pl.when(t == SECOND_SLOT)(lambda: self.gather.settle(2))

        def step(u, carry):
            j = (t - SECOND_SLOT) * PER_SLOT + u
            i = j - self.total
            pl.when(jnp.logical_and(j >= 0, i < 0))(lambda: self.down_piece(0, j))
            pl.when(i == 0)(lambda: self.await_parts(0))
            pl.when(jnp.logical_and(i >= 0, i < self.blocks))(lambda: self.update(0, i, 0.5))
            return carry

        lax.fori_loop(0, PER_SLOT, step, 0)

    def third_work(self, t):
        blocks = 2 * self.half // CONV_BLOCK

        def step(u, carry):
            j = (t - THIRD_SLOT) * PER_SLOT + u
            i = j - 2

            @pl.when(jnp.logical_or(j == 0, j == 1))
            def _():
                pl.when(j == 0)(lambda: self.gather.settle(3))
                pl.when(j == 1)(lambda: self.await_rows(1))
                self.gated(pl.multiple_of(jnp.where(j == 0, self.mine, self.theirs), self.half))

            pl.when(jnp.logical_and(i >= 0, i < blocks))(lambda: self.convolve(i))
            pl.when(i == blocks)(lambda: self.sum_copy().start())
            i = i - blocks - SUM_WAIT
            pl.when(i == 0)(lambda: self.sum_copy().wait_recv())
            pl.when(jnp.logical_and(i >= 0, i < blocks))(lambda: self.activate(i))
            return carry

        lax.fori_loop(0, PER_SLOT, step, 0)

    def gated(self, row):
        rows = self.rows[1, pl.ds(row, self.half), :]
        whole = self.gather.slots[3]
        height = whole.shape[1] // 2
        value = whole[:, :height, :].reshape(self.width, -1)
        gate = whole[:, height:, :].reshape(self.width, -1)
        values = jnp.dot(rows, value, preferred_element_type=jnp.float32)
        gates = jnp.dot(rows, gate, preferred_element_type=jnp.float32)
        self.padded[pl.ds(PAD + row, self.half), :] = values * jax.nn.sigmoid(gates)

    def convolve(self, i):
        taps = self.taps.shape[0]
        lanes = self.sums.shape[-1]
        first = pl.multiple_of(i * CONV_BLOCK, CONV_BLOCK)
        window = self.padded[pl.ds(first, CONV_BLOCK + PAD), :]
        channels = window.shape[1]
        total = jnp.zeros((CONV_BLOCK // SUBLANES, SUBLANES, channels), jnp.float32)
        offsets = [PAD - (taps - 1) + j for j in range(taps)]
        for shift in range(SUBLANES):
            mine = [(j, at) for j, at in enumerate(offsets) if at % SUBLANES == shift]
            reach = max(at for _, at in mine) - shift + CONV_BLOCK
            shifted = window[shift : shift + reach]
            for j, at in mine:
                block = shifted[at - shift : at - shift + CONV_BLOCK].reshape(total.shape)
                total = total + block * self.taps[j][None]
        total = total.reshape(CONV_BLOCK, channels)
        here = pl.ds(first, CONV_BLOCK)
        self.conv[here, :] = total
        plain = jnp.sum(total, axis=-1, keepdims=True)
        squared = jnp.sum(total * total, axis=-1, keepdims=True)
        lane = lax.broadcasted_iota(jnp.int32, (CONV_BLOCK, lanes), 1)
        self.sums[0, here, :] = jnp.where(lane < lanes // 2, plain, squared)

    def activate(self, i):
        lanes = self.sums.shape[-1]
        channels = 2 * self.conv.shape[1]
        here = pl.ds(pl.multiple_of(i * CONV_BLOCK, CONV_BLOCK), CONV_BLOCK)
        sums = (self.sums[0, here, :] + self.sums[1, here, :]) / channels
        average, square = sums[:, :1], sums[:, lanes // 2 : lanes // 2 + 1]
        spread = jnp.maximum(square - average * average, 0.0)
        scaled = (self.conv[here, :] - average) * lax.rsqrt(spread + CHAN_EPS)
        scaled = scaled.reshape(-1, SUBLANES, scaled.shape[1]) * self.gain[...][None]
        self.act[here, :] = jax.nn.silu(scaled.reshape(CONV_BLOCK, -1)).astype(jnp.bfloat16)

    def mix(self, row, k):
        rows, cols = pl.ds(row, self.half), pl.ds(pl.multiple_of(k * self.piece, self.piece), self.piece)
        result = jnp.dot(self.act[rows, :], self.columns(4, k), preferred_element_type=jnp.float32)
        self.partial[1, rows, cols] = result.astype(jnp.bfloat16)

    def finish_conv(self):
        self.gather.settle(4)

        def theirs(g, carry):
            group = [g * MIX_GROUP + u for u in range(MIX_GROUP)]
            for k in group:
                self.mix(self.theirs, k)
            for k in group:
                self.part_copy(1, k).start()
            return carry

        def mine(g, carry):
            for u in range(MIX_GROUP):
                self.mix(self.mine, g * MIX_GROUP + u)
            return carry

        lax.fori_loop(0, self.total // MIX_GROUP, theirs, 0)
        lax.fori_loop(0, self.total // MIX_GROUP, mine, 0)
        self.await_parts(1)

        def step(i, carry):
            self.update(1, i, None)
            return carry

        lax.fori_loop(0, self.blocks, step, 0)

    def second_half_step(self):
        tile = 2 * LANES
        whole = self.units // tile
        early = min(2, whole)

        def split(i, carry):
            pl.when(i == early)(lambda: self.await_rows(2))
            row = jnp.where(i < early, self.mine, self.theirs)
            first = pl.multiple_of(lax.rem(i, early) * tile, tile)
            self.hidden_tile(2, pl.multiple_of(row, self.half), self.half, first, tile)
            return carry

        lax.fori_loop(0, 2 * early, split, 0)

        def step(j, carry):
            self.hidden_tile(2, 0, 2 * self.half, pl.multiple_of(j * tile, tile), tile)
            return carry

        lax.fori_loop(early, whole, step, 0)
        if self.units % tile:
            self.hidden_tile(2, 0, 2 * self.half, whole * tile, self.units % tile)

        def down(row, k):
            return jnp.dot(self.hidden[pl.ds(row, self.half), :], self.columns(2, k), preferred_element_type=jnp.float32)

        def columns(k):
            return pl.ds(pl.multiple_of(k * self.piece, self.piece), self.piece)

        def theirs(g, carry):
            group = [g * DOWN_GROUP + u for u in range(DOWN_GROUP)]
            for k in group:
                self.partial[2, pl.ds(self.theirs, self.half), columns(k)] = down(self.theirs, k).astype(jnp.bfloat16)
            for k in group:
                self.part_copy(2, k).start()
            return carry

        def mine(g, carry):
            group = [g * DOWN_GROUP + u for u in range(DOWN_GROUP)]
            for k in group:
                self.part_copy(2, k).wait_recv()
            for k in group:
                cols = columns(k)
                own = down(self.mine, k).astype(jnp.bfloat16).astype(jnp.float32)
                added = own + self.landed[2, :, cols].astype(jnp.float32)
                self.mixed[:, cols] = (self.stream[:, cols] + 0.5 * added).astype(self.mixed.dtype)
            for k in group:
                cols = columns(k)
                pltpu.make_async_copy(self.mixed.at[:, cols], self.out.at[:, cols], self.out_sem.at[0]).start()
            return carry

        lax.fori_loop(0, self.total // DOWN_GROUP, theirs, 0)
        lax.fori_loop(0, self.total // DOWN_GROUP, mine, 0)

    def drain(self):
        self.sum_copy().wait_send()
        for n in range(3):
            self.row_copy(n, self.mine, self.half).wait_send()
            self.part_copy(n, 0, self.width).wait_send()

    def run(self):
        gather = self.gather
        gather.start_local()
        for load in self.loads:
            load.start()
        gather.barrier(self.partner)
        gather.start_own(0)
        for load in self.loads:
            load.wait()
        self.expand()
        self.start_rows()
        self.padded[:PAD, :] = jnp.zeros((PAD, self.padded.shape[1]), jnp.float32)
        gather.run(0)
        gather.run(1)
        gather.run(2, self.first_work)
        gather.run(3, self.second_work)
        gather.run(4, self.third_work)
        self.finish_conv()
        self.second_half_step()
        for m in range(len(gather.ins)):
            gather.drain(m)
        self.drain()
        pltpu.make_async_copy(self.mixed, self.out, self.out_sem.at[0]).wait()


def layer_kernel(depth, *refs):
    tokens, gains, taps, refs = refs[0], refs[1:5], refs[5], refs[6:]
    ins, refs = ((refs[0],), (refs[1],), (refs[2],), refs[3:5], (refs[5],)), refs[6:]
    out, refs = refs[0], refs[1:]
    slots, sems, scratch = refs[:5], refs[5:13], refs[13:]
    gather = Gather(depth, ins, slots, *sems[:3], sems[3:])
    Layer(gather, tokens, gains, taps, out, scratch).run()


def fused_layer(tokens, gains, depthwise, blocks, smalls):
    total = lax.axis_size("fs")
    half, width = tokens.shape
    units, (taps, channels) = blocks[0].shape[2], depthwise.shape
    vmem, dma = pltpu.VMEM, pltpu.SemaphoreType.DMA
    count, height, piece = smalls[0].shape
    shapes = [b.shape for b in blocks] + [(count, 2 * height, piece), (count, height, piece)]
    f32, bf16 = jnp.float32, jnp.bfloat16
    return pl.pallas_call(
        functools.partial(layer_kernel, total // 2),
        out_shape=jax.ShapeDtypeStruct((half, width), bf16),
        in_specs=[pl.BlockSpec(memory_space=pltpu.HBM)] * 12,
        out_specs=pl.BlockSpec(memory_space=pltpu.HBM),
        scratch_shapes=[vmem((total * shape[0], *shape[1:]), bf16) for shape in shapes]
        + gather_sems(total, 2, [shape[0] for shape in shapes])
        + [
            vmem((half, width), bf16),
            vmem((half, width), f32),
            vmem((3, 2 * half, width), bf16),
            vmem((2 * half, units), bf16),
            vmem((3, 2 * half, width), bf16),
            vmem((3, half, width), bf16),
            vmem((PAD + 2 * half, channels), f32),
            vmem((2 * half, channels), f32),
            vmem((2, 2 * half, LANES), f32),
            vmem((2 * half, channels), bf16),
            vmem((half, width), bf16),
        ]
        + [vmem(gain.shape, bf16) for gain in gains]
        + [
            vmem(depthwise.shape, bf16),
            vmem((3, SUBLANES, width), f32),
            vmem((SUBLANES, channels), f32),
            vmem((taps, SUBLANES, channels), f32),
            dma((6,)),
            dma((3,)),
            dma((3,)),
            dma((3,)),
            dma((2 + total,)),
            dma((1,)),
            dma((1,)),
            dma((1,)),
        ],
        compiler_params=pltpu.CompilerParams(
            collective_id=0, has_side_effects=True, vmem_limit_bytes=58 * 2**20
        ),
        name="fused_layer",
    )(tokens, *gains, depthwise, *blocks, *smalls)


def fits(half, ffn_gate, ffn_down, conv_value, conv_out, depthwise):
    piece, total = ffn_gate.shape[0], lax.axis_size("fs")
    slots, conv_slots = total // 2 * CHUNKS, total // 2 * CONV_CHUNKS
    return (
        piece % (16 * CHUNKS) == 0
        and ffn_down.shape[0] % (16 * CHUNKS) == 0
        and conv_out.shape[0] == piece
        and conv_value.shape[1] == piece
        and piece % LANES == 0
        and ffn_gate.shape[1] % LANES == 0
        and half % ROW_BLOCK == 0
        and half % CONV_BLOCK == 0
        and depthwise.shape[0] <= PAD
        and total % MIX_GROUP == 0
        and total % DOWN_GROUP == 0
        and slots >= FIRST_SLOT + ffn_gate.shape[1] // LANES
        and (conv_slots - SECOND_SLOT) * PER_SLOT >= total + half // ROW_BLOCK
        and (conv_slots - THIRD_SLOT) * PER_SLOT >= 2 + SUM_WAIT + 4 * half // CONV_BLOCK
        and lax.axis_size("tp") == 2
        and lax.axis_size("rep") == 2
    )


def shards(
    tokens,
    norm_first,
    norm_mixer,
    norm_second,
    ffn_gate,
    ffn_up,
    ffn_down,
    conv_value,
    conv_gate,
    depthwise,
    conv_gain,
    conv_out,
):
    width = tokens.shape[-1]
    if fits(tokens.size // width, ffn_gate, ffn_down, conv_value, conv_out, depthwise):
        mixed = fused_layer(
            tokens.reshape(-1, width),
            [gain.reshape(-1, LANES) for gain in (norm_first, norm_mixer, norm_second, conv_gain)],
            depthwise,
            [chunked(block, CHUNKS) for block in (ffn_gate, ffn_up, ffn_down)],
            [chunked(block, CONV_CHUNKS) for block in (conv_value, conv_gate, conv_out)],
        )
        return mixed.reshape(tokens.shape)
    stream = tokens.reshape(-1, width).astype(jnp.float32)
    first_rows = widen(rms_rows(stream, norm_first))
    small = jnp.concatenate([conv_value, conv_gate, conv_out.reshape(-1, conv_value.shape[1])])
    gate, up, down, small_all = gather_all(
        [chunked(block, CHUNKS) for block in (ffn_gate, ffn_up, ffn_down, small)]
    )
    whole_gate = gate.reshape(-1, gate.shape[-1])
    whole_up = up.reshape(-1, up.shape[-1])
    total = lax.axis_size("fs")
    whole_down = columns_of(down.reshape(total, -1, down.shape[-1]))
    small_all = small_all.reshape(total, -1, small_all.shape[-1])
    rows = conv_value.shape[0]
    channels_here = conv_value.shape[1]
    whole_value = small_all[:, :rows].reshape(-1, channels_here)
    whole_conv_gate = small_all[:, rows : 2 * rows].reshape(-1, channels_here)
    whole_out = columns_of(small_all[:, 2 * rows :].reshape(total, *conv_out.shape))

    hidden = hidden_units(first_rows, whole_gate, whole_up)
    stream = stream + 0.5 * narrow(jnp.dot(hidden, whole_down, preferred_element_type=jnp.float32))
    gathered = widen(rms_rows(stream, norm_mixer))
    values = jnp.dot(gathered, whole_value, preferred_element_type=jnp.float32)
    gates = jnp.dot(gathered, whole_conv_gate, preferred_element_type=jnp.float32)
    glu = reorder(values * jax.nn.sigmoid(gates))
    conv = causal_taps(glu, depthwise.astype(jnp.float32))
    channels = conv.shape[1] * lax.axis_size("tp")
    sums, squares = lax.psum((jnp.sum(conv, axis=1), jnp.sum(conv * conv, axis=1)), "tp")
    average = sums / channels
    spread = jnp.maximum(squares / channels - average * average, 0.0)
    centred = conv - average[:, None]
    activated = jax.nn.silu(
        centred * lax.rsqrt(spread[:, None] + CHAN_EPS) * conv_gain.astype(jnp.float32)
    ).astype(jnp.bfloat16)
    stream = stream + narrow(jnp.dot(reorder(activated), whole_out, preferred_element_type=jnp.float32))
    second_rows = widen(rms_rows(stream, norm_second))
    second_hidden = hidden_units(second_rows, whole_gate, whole_up)
    stream = stream + 0.5 * narrow(jnp.dot(second_hidden, whole_down, preferred_element_type=jnp.float32))
    return stream.astype(jnp.bfloat16).reshape(tokens.shape)


def solution(mesh):
    in_specs = (
        P(("rep", "fs"), "tp", None),
        P(),
        P(),
        P(),
        P("fs", "tp"),
        P("fs", "tp"),
        P("tp", "fs"),
        P("fs", "tp"),
        P("fs", "tp"),
        P(None, "tp"),
        P("tp"),
        P("tp", "fs"),
    )
    out_specs = P(("rep", "fs"), "tp", None)
    return jax.shard_map(shards, mesh=mesh, in_specs=in_specs, out_specs=out_specs, check_vma=False)
```

```python
import functools

import jax
import jax.numpy as jnp
from jax import lax
from jax.experimental import pallas as pl
from jax.experimental.pallas import tpu as pltpu
from jax.sharding import PartitionSpec as P

ROW_EPS = 0.05
CHAN_EPS = 0.02
MESH = pl.DeviceIdType.MESH
CHUNKS = 8
CONV_CHUNKS = 4
LANES = 128
ROW_BLOCK = 32
CONV_BLOCK = 64
PAD = 32
SUBLANES = 8
FIRST_SLOT = 8
SECOND_SLOT = 2
THIRD_SLOT = 2
PER_SLOT = 2
LARGE = 3
SUM_WAIT = 4
MIX_GROUP = 4
DOWN_GROUP = 2
UP, DOWN, OVER_X, OVER_Y = range(4)


def rms_rows(stream, gain_vec):
    square_mean = jnp.mean(stream * stream, axis=-1, keepdims=True)
    return (stream * lax.rsqrt(square_mean + ROW_EPS) * gain_vec.astype(jnp.float32)).astype(
        jnp.bfloat16
    )


def swap(value):
    size = lax.axis_size("tp")
    return lax.ppermute(value, "tp", [(i, size - 1 - i) for i in range(size)])


def widen(normed):
    return jnp.concatenate([normed, swap(normed)])


def narrow(partial_value):
    rounded = partial_value.astype(jnp.bfloat16)
    half = rounded.shape[0] // 2
    return rounded[:half].astype(jnp.float32) + swap(rounded[half:]).astype(jnp.float32)


def reorder(rows):
    half = rows.shape[0] // 2
    flipped = jnp.concatenate([rows[half:], rows[:half]])
    return jnp.where(lax.axis_index("tp") == 0, rows, flipped)


def place():
    fs = lax.axis_index("fs")
    return lax.axis_index("rep"), lax.rem(fs, 2), fs // 2


class Gather:
    def __init__(self, depth, ins, slots, local_sems, side_sems, send_sems, recv_sems):
        self.depth = depth
        self.ins, self.slots = ins, slots
        self.local_sems, self.recv_sems = local_sems, recv_sems
        self.side_sems, self.send_sems = side_sems, send_sems
        self.x, self.y, self.z = place()
        self.has_up, self.has_down = self.z + 1 < depth, self.z > 0
        self.own = self.z * 2 + self.y

    def target(self, way):
        if way == UP:
            return {"fs": (self.z + 1) * 2 + self.y}
        if way == DOWN:
            return {"fs": (self.z - 1) * 2 + self.y}
        if way == OVER_X:
            return {"rep": 1 - self.x}
        return {"fs": self.z * 2 + 1 - self.y}

    def barrier(self, *others):
        barrier = pltpu.get_barrier_semaphore()
        for target in (self.target(OVER_X), self.target(OVER_Y), *others):
            pl.semaphore_signal(barrier, inc=1, device_id=target, device_id_type=MESH)
        for way, present in ((UP, self.has_up), (DOWN, self.has_down)):

            @pl.when(present)
            def _(way=way):
                pl.semaphore_signal(barrier, inc=1, device_id=self.target(way), device_id_type=MESH)

        peers = 2 + len(others) + self.has_up.astype(jnp.int32) + self.has_down.astype(jnp.int32)
        pl.semaphore_wait(barrier, peers)

    def count(self, m):
        return self.slots[m].shape[0] // (2 * self.depth)

    def at_end(self, at):
        return jnp.logical_or(at == 0, at == self.depth - 1)

    def least(self, m):
        count = self.count(m)
        return count - count // 4 if m < LARGE else count

    def near(self, m):
        return 1 if m < LARGE else 2

    def along(self, m, at):
        return jnp.where(self.at_end(at), self.least(m), self.count(m))

    def across(self, m, d):
        count = self.count(m)
        far = jnp.clip(count // 2 + d - self.near(m), count // 2, count - count // 4)
        return jnp.where(self.at_end(self.z), far, count // 2)

    def chunk(self, m, k, e):
        count = self.count(m)
        return k * count + e + self.x * (count - 1 - 2 * e)

    def locals(self, m):
        copies, first = [], 0
        for n, part in enumerate(self.ins[m]):
            height = part.shape[1]
            count = self.count(m)
            here = self.slots[m].at[pl.ds(self.own * count, count), pl.ds(first, height)]
            copies.append(pltpu.make_async_copy(part, here, self.local_sems.at[m, n]))
            first += height
        return copies

    def copy(self, m, c, way):
        piece = self.slots[m].at[c]
        recv_sem = self.side_sems.at[m] if way == OVER_X else self.recv_sems[m].at[c]
        return pltpu.make_async_remote_copy(
            src_ref=piece,
            dst_ref=piece,
            send_sem=self.send_sems.at[m, way],
            recv_sem=recv_sem,
            device_id=self.target(way),
            device_id_type=MESH,
        )

    def spread(self, m, k, e, ways):
        c = self.chunk(m, k, e)
        for way, wanted in ways:
            pl.when(wanted)(lambda way=way: self.copy(m, c, way).start())

    def start_local(self):
        for m in range(len(self.ins)):
            for part in self.locals(m):
                part.start()

    def start_own(self, m):
        for part in self.locals(m):
            part.wait()
        up, down = self.along(m, self.z + 1), self.along(m, self.z - 1)
        across = self.across(m, 0)

        def step(e, carry):
            self.spread(
                m,
                self.own,
                e,
                (
                    (UP, jnp.logical_and(self.has_up, e < up)),
                    (DOWN, jnp.logical_and(self.has_down, e < down)),
                    (OVER_Y, e < across),
                ),
            )
            return carry

        lax.fori_loop(0, self.count(m), step, 0)

    def pieces(self, d):
        below, above = self.z - d, self.z + d
        return (
            (below, below >= 0, self.z + 1, self.has_up, UP),
            (above, jnp.logical_and(d > 0, above < self.depth), self.z - 1, self.has_down, DOWN),
        )

    def arrive_along(self, m, d, e):
        along, across = self.along(m, self.z), self.across(m, d)
        spare = self.count(m) - along
        for at, present, goal, further, way in self.pieces(d):

            @pl.when(jnp.logical_and(present, e < along))
            def _(at=at, goal=goal, further=further, way=way):
                k = at * 2 + self.y
                self.copy(m, self.chunk(m, k, e), UP).wait_recv()
                onward = jnp.logical_and(further, e < self.along(m, goal))
                self.spread(m, k, e, ((way, onward), (OVER_Y, e < across), (OVER_X, e < spare)))

    def arrive_across(self, m, d, e):
        across = self.across(m, d)
        spare = self.count(m) - across
        for at, present, _, _, _ in self.pieces(d):

            @pl.when(jnp.logical_and(present, e < across))
            def _(at=at):
                k = at * 2 + 1 - self.y
                self.copy(m, self.chunk(m, k, e), OVER_Y).wait_recv()
                self.spread(m, k, e, ((OVER_X, e < spare),))

    def slots_of(self, m):
        return self.depth * self.count(m)

    def run(self, m, work=None):
        count = self.count(m)
        ahead = min(self.depth - 1, 1 if m >= LARGE else self.depth) * count

        def step(t, carry):
            r, e = lax.div(t, count), lax.rem(t, count)
            if m + 1 < len(self.ins):
                pl.when(t == ahead)(lambda: self.start_own(m + 1))
            self.arrive_along(m, r + 1, e)
            self.arrive_across(m, r, e)
            if work is not None:
                work(t)
            return carry

        lax.fori_loop(0, self.slots_of(m), step, 0)

    def totals(self, m, z):
        count, last = self.count(m), self.depth - 1
        least = self.least(m)

        def along(at):
            return least if at in (0, last) else count

        def across(d):
            far = min(max(count // 2 + d - self.near(m), count // 2), count - count // 4)
            return far if z in (0, last) else count // 2

        distances = [0, *range(1, z + 1), *range(1, last - z + 1)]
        totals = [0] * 4
        if z < last:
            totals[UP] = along(z + 1) + z * min(along(z), along(z + 1))
        if z > 0:
            totals[DOWN] = along(z - 1) + (last - z) * min(along(z), along(z - 1))
        totals[OVER_Y] = sum(across(d) for d in distances)
        totals[OVER_X] = last * (count - along(z)) + sum(count - across(d) for d in distances)
        return totals

    def all_of(self, m, way, size):
        chunks = self.slots[m].at[pl.ds(0, size)]
        return pltpu.make_async_remote_copy(
            src_ref=chunks,
            dst_ref=chunks,
            send_sem=self.send_sems.at[m, way],
            recv_sem=self.side_sems.at[m],
            device_id=self.target(way),
            device_id_type=MESH,
        )

    def each_place(self, visit):
        for z in range(self.depth):
            pl.when(self.z == z)(lambda z=z: visit(z))

    def settle(self, m):
        self.each_place(lambda z: self.all_of(m, OVER_X, self.totals(m, z)[OVER_X]).wait_recv())

    def drain(self, m):
        def visit(z):
            for way, size in enumerate(self.totals(m, z)):
                if size:
                    self.all_of(m, way, size).wait_send()

        self.each_place(visit)


def gather_sems(total, parts, counts):
    dma = pltpu.SemaphoreType.DMA
    return [dma((len(counts), parts)), dma((len(counts),)), dma((len(counts), 4))] + [
        dma((total * count,)) for count in counts
    ]


def gather_kernel(depth, count, *refs):
    ins, slots = [(ref,) for ref in refs[:count]], refs[count : 2 * count]
    sems = refs[2 * count :]
    gather = Gather(depth, ins, slots, *sems[:3], sems[3:])
    gather.start_local()
    gather.barrier()
    gather.start_own(0)
    for m in range(count):
        gather.run(m)
    for m in range(count):
        gather.settle(m)
        gather.drain(m)


def gather_all(blocks):
    total = lax.axis_size("fs")
    count = len(blocks)
    outs = [jax.ShapeDtypeStruct((total * b.shape[0], *b.shape[1:]), b.dtype) for b in blocks]
    return pl.pallas_call(
        functools.partial(gather_kernel, total // 2, count),
        out_shape=outs,
        in_specs=[pl.BlockSpec(memory_space=pl.ANY)] * count,
        out_specs=[pl.BlockSpec(memory_space=pltpu.VMEM)] * count,
        scratch_shapes=gather_sems(total, 1, [b.shape[0] for b in blocks]),
        compiler_params=pltpu.CompilerParams(
            collective_id=0, has_side_effects=True, vmem_limit_bytes=48 * 2**20
        ),
        name="gather_all",
    )(*blocks)


def hidden_units(gathered, whole_gate, whole_up):
    gate_rows = jnp.dot(gathered, whole_gate, preferred_element_type=jnp.float32)
    up_rows = jnp.dot(gathered, whole_up, preferred_element_type=jnp.float32)
    return (jax.nn.silu(gate_rows) * up_rows).astype(jnp.bfloat16)


def columns_of(blocks):
    return blocks.transpose(1, 0, 2).reshape(blocks.shape[1], -1)


def causal_taps(glu, kernel):
    length = glu.shape[0]
    taps = kernel.shape[0]
    padded = jnp.pad(glu, ((taps - 1, 0), (0, 0)))
    output = jnp.zeros_like(glu)
    for tap_index in range(taps):
        output = output + padded[tap_index : tap_index + length] * kernel[tap_index]
    return output


def chunked(block, pieces):
    return block.reshape(pieces, block.shape[0] // pieces, block.shape[1])


class Layer:
    def __init__(self, gather, tokens, gains, taps, out, scratch):
        self.gather = gather
        self.out = out
        (
            self.own,
            self.stream,
            self.rows,
            self.hidden,
            self.partial,
            self.landed,
            self.padded,
            self.conv,
            self.sums,
            self.act,
            self.mixed,
            *self.packed,
            self.packed_taps,
            self.gains,
            self.gain,
            self.taps,
            self.own_sems,
            self.row_send,
            self.row_recv,
            self.part_send,
            self.part_recv,
            self.sum_send,
            self.sum_recv,
            self.out_sem,
        ) = scratch
        self.half, self.width = self.own.shape
        self.units = self.hidden.shape[1]
        self.total = gather.depth * 2
        self.piece = self.width // self.total
        self.blocks = self.half // ROW_BLOCK
        self.tp = lax.axis_index("tp")
        self.partner = {"tp": 1 - self.tp}
        self.mine = pl.multiple_of(self.tp * self.half, self.half)
        self.theirs = pl.multiple_of((1 - self.tp) * self.half, self.half)
        inputs = (tokens, *gains, taps)
        self.loads = [
            pltpu.make_async_copy(src, dst, self.own_sems.at[n])
            for n, (src, dst) in enumerate(zip(inputs, (self.own, *self.packed, self.packed_taps)))
        ]

    def expand(self):
        for n, packed in enumerate(self.packed):
            target = self.gain if n == 3 else self.gains.at[n]
            for j in range(packed.shape[0]):
                row = packed[j : j + 1, :].astype(jnp.float32)
                target[:, j * LANES : (j + 1) * LANES] = jnp.broadcast_to(row, (SUBLANES, LANES))
        for j in range(self.taps.shape[0]):
            row = self.packed_taps[j : j + 1, :].astype(jnp.float32)
            self.taps[j] = jnp.broadcast_to(row, (SUBLANES, row.shape[1]))

    def remote(self, src, dst, send_sem, recv_sem):
        return pltpu.make_async_remote_copy(
            src_ref=src,
            dst_ref=dst,
            send_sem=send_sem,
            recv_sem=recv_sem,
            device_id=self.partner,
            device_id_type=MESH,
        )

    def row_copy(self, n, first, count):
        here = self.rows.at[n, pl.ds(first, count)]
        return self.remote(here, here, self.row_send.at[n], self.row_recv.at[n])

    def await_rows(self, n):
        self.row_copy(n, self.theirs, self.half).wait_recv()

    def part_copy(self, n, k, width=None):
        cols = pl.ds(pl.multiple_of(k * self.piece, self.piece), self.piece if width is None else width)
        return self.remote(
            self.partial.at[n, pl.ds(self.theirs, self.half), cols],
            self.landed.at[n, :, cols],
            self.part_send.at[n],
            self.part_recv.at[n + (k if n == 2 else 0)],
        )

    def sum_copy(self):
        return self.remote(self.sums.at[0], self.sums.at[1], self.sum_send.at[0], self.sum_recv.at[0])

    def norm(self, n, i, stream):
        square_mean = jnp.mean(stream * stream, axis=-1, keepdims=True)
        scaled = (stream * lax.rsqrt(square_mean + ROW_EPS)).reshape(-1, SUBLANES, self.width) * self.gains[n][None]
        rows = pl.ds(self.mine + self.block(i), ROW_BLOCK)
        self.rows[n, rows, :] = scaled.reshape(stream.shape).astype(jnp.bfloat16)
        self.row_copy(n, self.mine + self.block(i), ROW_BLOCK).start()

    def block(self, i):
        return pl.multiple_of(i * ROW_BLOCK, ROW_BLOCK)

    def start_rows(self):
        def step(i, carry):
            self.norm(0, i, self.own[pl.ds(self.block(i), ROW_BLOCK), :].astype(jnp.float32))
            return carry

        lax.fori_loop(0, self.blocks, step, 0)

    def update(self, n, i, scale):
        first = self.block(i)
        here = pl.ds(first, ROW_BLOCK)
        before = self.own[here, :].astype(jnp.float32) if n == 0 else self.stream[here, :]
        added = self.partial[n, pl.ds(self.mine + first, ROW_BLOCK), :].astype(jnp.float32) + self.landed[
            n, here, :
        ].astype(jnp.float32)
        stream = before + (added if scale is None else scale * added)
        self.stream[here, :] = stream
        self.norm(n + 1, i, stream)

    def await_parts(self, n):
        self.part_copy(n, 0, self.width).wait_recv()

    def matrix(self, m, first, size):
        return self.gather.slots[m][:, :, pl.ds(first, size)].reshape(self.width, size)

    def columns(self, m, k):
        count = self.gather.count(m)
        return self.gather.slots[m][pl.ds(k * count, count)].reshape(-1, self.piece)

    def hidden_tile(self, n, row, height, first, size):
        rows = self.rows[n, pl.ds(row, height), :]
        gate = jnp.dot(rows, self.matrix(0, first, size), preferred_element_type=jnp.float32)
        up = jnp.dot(rows, self.matrix(1, first, size), preferred_element_type=jnp.float32)
        self.hidden[pl.ds(row, height), pl.ds(first, size)] = (jax.nn.silu(gate) * up).astype(jnp.bfloat16)

    def down_piece(self, n, k):
        weights = self.columns(2, k)
        result = jnp.dot(self.hidden[...], weights, preferred_element_type=jnp.float32)
        cols = pl.ds(pl.multiple_of(k * self.piece, self.piece), self.piece)
        self.partial[n, :, cols] = result.astype(jnp.bfloat16)
        self.part_copy(n, k).start()

    def first_work(self, t):
        j = t - FIRST_SLOT

        @pl.when(j == 0)
        def _():
            self.gather.settle(0)
            self.gather.settle(1)
            self.await_rows(0)

        @pl.when(jnp.logical_and(j >= 0, j < self.units // LANES))
        def _():
            self.hidden_tile(0, 0, 2 * self.half, pl.multiple_of(j * LANES, LANES), LANES)

    def second_work(self, t):
        pl.when(t == SECOND_SLOT)(lambda: self.gather.settle(2))

        def step(u, carry):
            j = (t - SECOND_SLOT) * PER_SLOT + u
            i = j - self.total
            pl.when(jnp.logical_and(j >= 0, i < 0))(lambda: self.down_piece(0, j))
            pl.when(i == 0)(lambda: self.await_parts(0))
            pl.when(jnp.logical_and(i >= 0, i < self.blocks))(lambda: self.update(0, i, 0.5))
            return carry

        lax.fori_loop(0, PER_SLOT, step, 0)

    def third_work(self, t):
        blocks = 2 * self.half // CONV_BLOCK

        def step(u, carry):
            j = (t - THIRD_SLOT) * PER_SLOT + u
            i = j - 2

            @pl.when(jnp.logical_or(j == 0, j == 1))
            def _():
                pl.when(j == 0)(lambda: self.gather.settle(3))
                pl.when(j == 1)(lambda: self.await_rows(1))
                self.gated(pl.multiple_of(jnp.where(j == 0, self.mine, self.theirs), self.half))

            pl.when(jnp.logical_and(i >= 0, i < blocks))(lambda: self.convolve(i))
            pl.when(i == blocks)(lambda: self.sum_copy().start())
            i = i - blocks - SUM_WAIT
            pl.when(i == 0)(lambda: self.sum_copy().wait_recv())
            pl.when(jnp.logical_and(i >= 0, i < blocks))(lambda: self.activate(i))
            return carry

        lax.fori_loop(0, PER_SLOT, step, 0)

    def gated(self, row):
        rows = self.rows[1, pl.ds(row, self.half), :]
        whole = self.gather.slots[3]
        height = whole.shape[1] // 2
        value = whole[:, :height, :].reshape(self.width, -1)
        gate = whole[:, height:, :].reshape(self.width, -1)
        values = jnp.dot(rows, value, preferred_element_type=jnp.float32)
        gates = jnp.dot(rows, gate, preferred_element_type=jnp.float32)
        self.padded[pl.ds(PAD + row, self.half), :] = values * jax.nn.sigmoid(gates)

    def convolve(self, i):
        taps = self.taps.shape[0]
        lanes = self.sums.shape[-1]
        first = pl.multiple_of(i * CONV_BLOCK, CONV_BLOCK)
        window = self.padded[pl.ds(first, CONV_BLOCK + PAD), :]
        channels = window.shape[1]
        total = jnp.zeros((CONV_BLOCK // SUBLANES, SUBLANES, channels), jnp.float32)
        offsets = [PAD - (taps - 1) + j for j in range(taps)]
        for shift in range(SUBLANES):
            mine = [(j, at) for j, at in enumerate(offsets) if at % SUBLANES == shift]
            reach = max(at for _, at in mine) - shift + CONV_BLOCK
            shifted = window[shift : shift + reach]
            for j, at in mine:
                block = shifted[at - shift : at - shift + CONV_BLOCK].reshape(total.shape)
                total = total + block * self.taps[j][None]
        total = total.reshape(CONV_BLOCK, channels)
        here = pl.ds(first, CONV_BLOCK)
        self.conv[here, :] = total
        plain = jnp.sum(total, axis=-1, keepdims=True)
        squared = jnp.sum(total * total, axis=-1, keepdims=True)
        lane = lax.broadcasted_iota(jnp.int32, (CONV_BLOCK, lanes), 1)
        self.sums[0, here, :] = jnp.where(lane < lanes // 2, plain, squared)

    def activate(self, i):
        lanes = self.sums.shape[-1]
        channels = 2 * self.conv.shape[1]
        here = pl.ds(pl.multiple_of(i * CONV_BLOCK, CONV_BLOCK), CONV_BLOCK)
        sums = (self.sums[0, here, :] + self.sums[1, here, :]) / channels
        average, square = sums[:, :1], sums[:, lanes // 2 : lanes // 2 + 1]
        spread = jnp.maximum(square - average * average, 0.0)
        scaled = (self.conv[here, :] - average) * lax.rsqrt(spread + CHAN_EPS)
        scaled = scaled.reshape(-1, SUBLANES, scaled.shape[1]) * self.gain[...][None]
        self.act[here, :] = jax.nn.silu(scaled.reshape(CONV_BLOCK, -1)).astype(jnp.bfloat16)

    def mix(self, row, k):
        rows, cols = pl.ds(row, self.half), pl.ds(pl.multiple_of(k * self.piece, self.piece), self.piece)
        result = jnp.dot(self.act[rows, :], self.columns(4, k), preferred_element_type=jnp.float32)
        self.partial[1, rows, cols] = result.astype(jnp.bfloat16)

    def finish_conv(self):
        self.gather.settle(4)

        def theirs(g, carry):
            group = [g * MIX_GROUP + u for u in range(MIX_GROUP)]
            for k in group:
                self.mix(self.theirs, k)
            for k in group:
                self.part_copy(1, k).start()
            return carry

        def mine(g, carry):
            for u in range(MIX_GROUP):
                self.mix(self.mine, g * MIX_GROUP + u)
            return carry

        lax.fori_loop(0, self.total // MIX_GROUP, theirs, 0)
        lax.fori_loop(0, self.total // MIX_GROUP, mine, 0)
        self.await_parts(1)

        def step(i, carry):
            self.update(1, i, None)
            return carry

        lax.fori_loop(0, self.blocks, step, 0)

    def second_half_step(self):
        tile = 2 * LANES
        whole = self.units // tile
        early = min(2, whole)

        def split(i, carry):
            pl.when(i == early)(lambda: self.await_rows(2))
            row = jnp.where(i < early, self.mine, self.theirs)
            first = pl.multiple_of(lax.rem(i, early) * tile, tile)
            self.hidden_tile(2, pl.multiple_of(row, self.half), self.half, first, tile)
            return carry

        lax.fori_loop(0, 2 * early, split, 0)

        def step(j, carry):
            self.hidden_tile(2, 0, 2 * self.half, pl.multiple_of(j * tile, tile), tile)
            return carry

        lax.fori_loop(early, whole, step, 0)
        if self.units % tile:
            self.hidden_tile(2, 0, 2 * self.half, whole * tile, self.units % tile)

        def down(row, k):
            return jnp.dot(self.hidden[pl.ds(row, self.half), :], self.columns(2, k), preferred_element_type=jnp.float32)

        def columns(k):
            return pl.ds(pl.multiple_of(k * self.piece, self.piece), self.piece)

        def theirs(g, carry):
            group = [g * DOWN_GROUP + u for u in range(DOWN_GROUP)]
            for k in group:
                self.partial[2, pl.ds(self.theirs, self.half), columns(k)] = down(self.theirs, k).astype(jnp.bfloat16)
            for k in group:
                self.part_copy(2, k).start()
            return carry

        def mine(g, carry):
            group = [g * DOWN_GROUP + u for u in range(DOWN_GROUP)]
            for k in group:
                self.part_copy(2, k).wait_recv()
            for k in group:
                cols = columns(k)
                own = down(self.mine, k).astype(jnp.bfloat16).astype(jnp.float32)
                added = own + self.landed[2, :, cols].astype(jnp.float32)
                self.mixed[:, cols] = (self.stream[:, cols] + 0.5 * added).astype(self.mixed.dtype)
            for k in group:
                cols = columns(k)
                pltpu.make_async_copy(self.mixed.at[:, cols], self.out.at[:, cols], self.out_sem.at[0]).start()
            return carry

        lax.fori_loop(0, self.total // DOWN_GROUP, theirs, 0)
        lax.fori_loop(0, self.total // DOWN_GROUP, mine, 0)

    def drain(self):
        self.sum_copy().wait_send()
        for n in range(3):
            self.row_copy(n, self.mine, self.half).wait_send()
            self.part_copy(n, 0, self.width).wait_send()

    def run(self):
        gather = self.gather
        gather.start_local()
        for load in self.loads:
            load.start()
        gather.barrier(self.partner)
        gather.start_own(0)
        for load in self.loads:
            load.wait()
        self.expand()
        self.start_rows()
        self.padded[:PAD, :] = jnp.zeros((PAD, self.padded.shape[1]), jnp.float32)
        gather.run(0)
        gather.run(1)
        gather.run(2, self.first_work)
        gather.run(3, self.second_work)
        gather.run(4, self.third_work)
        self.finish_conv()
        self.second_half_step()
        for m in range(len(gather.ins)):
            gather.drain(m)
        self.drain()
        pltpu.make_async_copy(self.mixed, self.out, self.out_sem.at[0]).wait()


def layer_kernel(depth, *refs):
    tokens, gains, taps, refs = refs[0], refs[1:5], refs[5], refs[6:]
    ins, refs = ((refs[0],), (refs[1],), (refs[2],), refs[3:5], (refs[5],)), refs[6:]
    out, refs = refs[0], refs[1:]
    slots, sems, scratch = refs[:5], refs[5:13], refs[13:]
    gather = Gather(depth, ins, slots, *sems[:3], sems[3:])
    Layer(gather, tokens, gains, taps, out, scratch).run()


def fused_layer(tokens, gains, depthwise, blocks, smalls):
    total = lax.axis_size("fs")
    half, width = tokens.shape
    units, (taps, channels) = blocks[0].shape[2], depthwise.shape
    vmem, dma = pltpu.VMEM, pltpu.SemaphoreType.DMA
    count, height, piece = smalls[0].shape
    shapes = [b.shape for b in blocks] + [(count, 2 * height, piece), (count, height, piece)]
    f32, bf16 = jnp.float32, jnp.bfloat16
    return pl.pallas_call(
        functools.partial(layer_kernel, total // 2),
        out_shape=jax.ShapeDtypeStruct((half, width), bf16),
        in_specs=[pl.BlockSpec(memory_space=pltpu.HBM)] * 12,
        out_specs=pl.BlockSpec(memory_space=pltpu.HBM),
        scratch_shapes=[vmem((total * shape[0], *shape[1:]), bf16) for shape in shapes]
        + gather_sems(total, 2, [shape[0] for shape in shapes])
        + [
            vmem((half, width), bf16),
            vmem((half, width), f32),
            vmem((3, 2 * half, width), bf16),
            vmem((2 * half, units), bf16),
            vmem((3, 2 * half, width), bf16),
            vmem((3, half, width), bf16),
            vmem((PAD + 2 * half, channels), f32),
            vmem((2 * half, channels), f32),
            vmem((2, 2 * half, LANES), f32),
            vmem((2 * half, channels), bf16),
            vmem((half, width), bf16),
        ]
        + [vmem(gain.shape, bf16) for gain in gains]
        + [
            vmem(depthwise.shape, bf16),
            vmem((3, SUBLANES, width), f32),
            vmem((SUBLANES, channels), f32),
            vmem((taps, SUBLANES, channels), f32),
            dma((6,)),
            dma((3,)),
            dma((3,)),
            dma((3,)),
            dma((2 + total,)),
            dma((1,)),
            dma((1,)),
            dma((1,)),
        ],
        compiler_params=pltpu.CompilerParams(
            collective_id=0, has_side_effects=True, vmem_limit_bytes=58 * 2**20
        ),
        name="fused_layer",
    )(tokens, *gains, depthwise, *blocks, *smalls)


def fits(half, ffn_gate, ffn_down, conv_value, conv_out, depthwise):
    piece, total = ffn_gate.shape[0], lax.axis_size("fs")
    slots, conv_slots = total // 2 * CHUNKS, total // 2 * CONV_CHUNKS
    return (
        piece % (16 * CHUNKS) == 0
        and ffn_down.shape[0] % (16 * CHUNKS) == 0
        and conv_out.shape[0] == piece
        and conv_value.shape[1] == piece
        and piece % LANES == 0
        and ffn_gate.shape[1] % LANES == 0
        and half % ROW_BLOCK == 0
        and half % CONV_BLOCK == 0
        and depthwise.shape[0] <= PAD
        and total % MIX_GROUP == 0
        and total % DOWN_GROUP == 0
        and slots >= FIRST_SLOT + ffn_gate.shape[1] // LANES
        and (conv_slots - SECOND_SLOT) * PER_SLOT >= total + half // ROW_BLOCK
        and (conv_slots - THIRD_SLOT) * PER_SLOT >= 2 + SUM_WAIT + 4 * half // CONV_BLOCK
        and lax.axis_size("tp") == 2
        and lax.axis_size("rep") == 2
    )


def shards(
    tokens,
    norm_first,
    norm_mixer,
    norm_second,
    ffn_gate,
    ffn_up,
    ffn_down,
    conv_value,
    conv_gate,
    depthwise,
    conv_gain,
    conv_out,
):
    width = tokens.shape[-1]
    if fits(tokens.size // width, ffn_gate, ffn_down, conv_value, conv_out, depthwise):
        mixed = fused_layer(
            tokens.reshape(-1, width),
            [gain.reshape(-1, LANES) for gain in (norm_first, norm_mixer, norm_second, conv_gain)],
            depthwise,
            [chunked(block, CHUNKS) for block in (ffn_gate, ffn_up, ffn_down)],
            [chunked(block, CONV_CHUNKS) for block in (conv_value, conv_gate, conv_out)],
        )
        return mixed.reshape(tokens.shape)
    stream = tokens.reshape(-1, width).astype(jnp.float32)
    first_rows = widen(rms_rows(stream, norm_first))
    small = jnp.concatenate([conv_value, conv_gate, conv_out.reshape(-1, conv_value.shape[1])])
    gate, up, down, small_all = gather_all(
        [chunked(block, CHUNKS) for block in (ffn_gate, ffn_up, ffn_down, small)]
    )
    whole_gate = gate.reshape(-1, gate.shape[-1])
    whole_up = up.reshape(-1, up.shape[-1])
    total = lax.axis_size("fs")
    whole_down = columns_of(down.reshape(total, -1, down.shape[-1]))
    small_all = small_all.reshape(total, -1, small_all.shape[-1])
    rows = conv_value.shape[0]
    channels_here = conv_value.shape[1]
    whole_value = small_all[:, :rows].reshape(-1, channels_here)
    whole_conv_gate = small_all[:, rows : 2 * rows].reshape(-1, channels_here)
    whole_out = columns_of(small_all[:, 2 * rows :].reshape(total, *conv_out.shape))

    hidden = hidden_units(first_rows, whole_gate, whole_up)
    stream = stream + 0.5 * narrow(jnp.dot(hidden, whole_down, preferred_element_type=jnp.float32))
    gathered = widen(rms_rows(stream, norm_mixer))
    values = jnp.dot(gathered, whole_value, preferred_element_type=jnp.float32)
    gates = jnp.dot(gathered, whole_conv_gate, preferred_element_type=jnp.float32)
    glu = reorder(values * jax.nn.sigmoid(gates))
    conv = causal_taps(glu, depthwise.astype(jnp.float32))
    channels = conv.shape[1] * lax.axis_size("tp")
    sums, squares = lax.psum((jnp.sum(conv, axis=1), jnp.sum(conv * conv, axis=1)), "tp")
    average = sums / channels
    spread = jnp.maximum(squares / channels - average * average, 0.0)
    centred = conv - average[:, None]
    activated = jax.nn.silu(
        centred * lax.rsqrt(spread[:, None] + CHAN_EPS) * conv_gain.astype(jnp.float32)
    ).astype(jnp.bfloat16)
    stream = stream + narrow(jnp.dot(reorder(activated), whole_out, preferred_element_type=jnp.float32))
    second_rows = widen(rms_rows(stream, norm_second))
    second_hidden = hidden_units(second_rows, whole_gate, whole_up)
    stream = stream + 0.5 * narrow(jnp.dot(second_hidden, whole_down, preferred_element_type=jnp.float32))
    return stream.astype(jnp.bfloat16).reshape(tokens.shape)


def solution(mesh):
    in_specs = (
        P(("rep", "fs"), "tp", None),
        P(),
        P(),
        P(),
        P("fs", "tp"),
        P("fs", "tp"),
        P("tp", "fs"),
        P("fs", "tp"),
        P("fs", "tp"),
        P(None, "tp"),
        P("tp"),
        P("tp", "fs"),
    )
    out_specs = P(("rep", "fs"), "tp", None)
    return jax.shard_map(shards, mesh=mesh, in_specs=in_specs, out_specs=out_specs, check_vma=False)
```

```python
import functools

import jax
import jax.numpy as jnp
from jax import lax
from jax.experimental import pallas as pl
from jax.experimental.pallas import tpu as pltpu
from jax.sharding import PartitionSpec as P

ROW_EPS = 0.05
CHAN_EPS = 0.02
MESH = pl.DeviceIdType.MESH
CHUNKS = 8
CONV_CHUNKS = 4
LANES = 128
ROW_BLOCK = 32
CONV_BLOCK = 64
PAD = 32
SUBLANES = 8
FIRST_SLOT = 8
SECOND_SLOT = 2
THIRD_SLOT = 2
PER_SLOT = 2
LARGE = 3
SUM_WAIT = 4
MIX_GROUP = 4
DOWN_GROUP = 2
UP, DOWN, OVER_X, OVER_Y = range(4)


def rms_rows(stream, gain_vec):
    square_mean = jnp.mean(stream * stream, axis=-1, keepdims=True)
    return (stream * lax.rsqrt(square_mean + ROW_EPS) * gain_vec.astype(jnp.float32)).astype(
        jnp.bfloat16
    )


def swap(value):
    size = lax.axis_size("tp")
    return lax.ppermute(value, "tp", [(i, size - 1 - i) for i in range(size)])


def widen(normed):
    return jnp.concatenate([normed, swap(normed)])


def narrow(partial_value):
    rounded = partial_value.astype(jnp.bfloat16)
    half = rounded.shape[0] // 2
    return rounded[:half].astype(jnp.float32) + swap(rounded[half:]).astype(jnp.float32)


def reorder(rows):
    half = rows.shape[0] // 2
    flipped = jnp.concatenate([rows[half:], rows[:half]])
    return jnp.where(lax.axis_index("tp") == 0, rows, flipped)


def place():
    fs = lax.axis_index("fs")
    return lax.axis_index("rep"), lax.rem(fs, 2), fs // 2


class Gather:
    def __init__(self, depth, ins, slots, local_sems, side_sems, send_sems, recv_sems):
        self.depth = depth
        self.ins, self.slots = ins, slots
        self.local_sems, self.recv_sems = local_sems, recv_sems
        self.side_sems, self.send_sems = side_sems, send_sems
        self.x, self.y, self.z = place()
        self.has_up, self.has_down = self.z + 1 < depth, self.z > 0
        self.own = self.z * 2 + self.y

    def target(self, way):
        if way == UP:
            return {"fs": (self.z + 1) * 2 + self.y}
        if way == DOWN:
            return {"fs": (self.z - 1) * 2 + self.y}
        if way == OVER_X:
            return {"rep": 1 - self.x}
        return {"fs": self.z * 2 + 1 - self.y}

    def barrier(self, *others):
        barrier = pltpu.get_barrier_semaphore()
        for target in (self.target(OVER_X), self.target(OVER_Y), *others):
            pl.semaphore_signal(barrier, inc=1, device_id=target, device_id_type=MESH)
        for way, present in ((UP, self.has_up), (DOWN, self.has_down)):

            @pl.when(present)
            def _(way=way):
                pl.semaphore_signal(barrier, inc=1, device_id=self.target(way), device_id_type=MESH)

        peers = 2 + len(others) + self.has_up.astype(jnp.int32) + self.has_down.astype(jnp.int32)
        pl.semaphore_wait(barrier, peers)

    def count(self, m):
        return self.slots[m].shape[0] // (2 * self.depth)

    def at_end(self, at):
        return jnp.logical_or(at == 0, at == self.depth - 1)

    def least(self, m):
        count = self.count(m)
        return count - count // 4 if m < LARGE else count

    def near(self, m):
        return 1 if m < LARGE else 2

    def along(self, m, at):
        return jnp.where(self.at_end(at), self.least(m), self.count(m))

    def across(self, m, d):
        count = self.count(m)
        far = jnp.clip(count // 2 + d - self.near(m), count // 2, count - count // 4)
        return jnp.where(self.at_end(self.z), far, count // 2)

    def chunk(self, m, k, e):
        count = self.count(m)
        return k * count + e + self.x * (count - 1 - 2 * e)

    def locals(self, m):
        copies, first = [], 0
        for n, part in enumerate(self.ins[m]):
            height = part.shape[1]
            count = self.count(m)
            here = self.slots[m].at[pl.ds(self.own * count, count), pl.ds(first, height)]
            copies.append(pltpu.make_async_copy(part, here, self.local_sems.at[m, n]))
            first += height
        return copies

    def copy(self, m, c, way):
        piece = self.slots[m].at[c]
        recv_sem = self.side_sems.at[m] if way == OVER_X else self.recv_sems[m].at[c]
        return pltpu.make_async_remote_copy(
            src_ref=piece,
            dst_ref=piece,
            send_sem=self.send_sems.at[m, way],
            recv_sem=recv_sem,
            device_id=self.target(way),
            device_id_type=MESH,
        )

    def spread(self, m, k, e, ways):
        c = self.chunk(m, k, e)
        for way, wanted in ways:
            pl.when(wanted)(lambda way=way: self.copy(m, c, way).start())

    def start_local(self):
        for m in range(len(self.ins)):
            for part in self.locals(m):
                part.start()

    def start_own(self, m):
        for part in self.locals(m):
            part.wait()
        up, down = self.along(m, self.z + 1), self.along(m, self.z - 1)
        across = self.across(m, 0)

        def step(e, carry):
            self.spread(
                m,
                self.own,
                e,
                (
                    (UP, jnp.logical_and(self.has_up, e < up)),
                    (DOWN, jnp.logical_and(self.has_down, e < down)),
                    (OVER_Y, e < across),
                ),
            )
            return carry

        lax.fori_loop(0, self.count(m), step, 0)

    def pieces(self, d):
        below, above = self.z - d, self.z + d
        return (
            (below, below >= 0, self.z + 1, self.has_up, UP),
            (above, jnp.logical_and(d > 0, above < self.depth), self.z - 1, self.has_down, DOWN),
        )

    def arrive_along(self, m, d, e):
        along, across = self.along(m, self.z), self.across(m, d)
        spare = self.count(m) - along
        for at, present, goal, further, way in self.pieces(d):

            @pl.when(jnp.logical_and(present, e < along))
            def _(at=at, goal=goal, further=further, way=way):
                k = at * 2 + self.y
                self.copy(m, self.chunk(m, k, e), UP).wait_recv()
                onward = jnp.logical_and(further, e < self.along(m, goal))
                self.spread(m, k, e, ((way, onward), (OVER_Y, e < across), (OVER_X, e < spare)))

    def arrive_across(self, m, d, e):
        across = self.across(m, d)
        spare = self.count(m) - across
        for at, present, _, _, _ in self.pieces(d):

            @pl.when(jnp.logical_and(present, e < across))
            def _(at=at):
                k = at * 2 + 1 - self.y
                self.copy(m, self.chunk(m, k, e), OVER_Y).wait_recv()
                self.spread(m, k, e, ((OVER_X, e < spare),))

    def slots_of(self, m):
        return self.depth * self.count(m)

    def run(self, m, work=None):
        count = self.count(m)
        ahead = min(self.depth - 1, 1 if m >= LARGE else self.depth) * count

        def step(t, carry):
            r, e = lax.div(t, count), lax.rem(t, count)
            if m + 1 < len(self.ins):
                pl.when(t == ahead)(lambda: self.start_own(m + 1))
            self.arrive_along(m, r + 1, e)
            self.arrive_across(m, r, e)
            if work is not None:
                work(t)
            return carry

        lax.fori_loop(0, self.slots_of(m), step, 0)

    def totals(self, m, z):
        count, last = self.count(m), self.depth - 1
        least = self.least(m)

        def along(at):
            return least if at in (0, last) else count

        def across(d):
            far = min(max(count // 2 + d - self.near(m), count // 2), count - count // 4)
            return far if z in (0, last) else count // 2

        distances = [0, *range(1, z + 1), *range(1, last - z + 1)]
        totals = [0] * 4
        if z < last:
            totals[UP] = along(z + 1) + z * min(along(z), along(z + 1))
        if z > 0:
            totals[DOWN] = along(z - 1) + (last - z) * min(along(z), along(z - 1))
        totals[OVER_Y] = sum(across(d) for d in distances)
        totals[OVER_X] = last * (count - along(z)) + sum(count - across(d) for d in distances)
        return totals

    def all_of(self, m, way, size):
        chunks = self.slots[m].at[pl.ds(0, size)]
        return pltpu.make_async_remote_copy(
            src_ref=chunks,
            dst_ref=chunks,
            send_sem=self.send_sems.at[m, way],
            recv_sem=self.side_sems.at[m],
            device_id=self.target(way),
            device_id_type=MESH,
        )

    def each_place(self, visit):
        for z in range(self.depth):
            pl.when(self.z == z)(lambda z=z: visit(z))

    def settle(self, m):
        self.each_place(lambda z: self.all_of(m, OVER_X, self.totals(m, z)[OVER_X]).wait_recv())

    def drain(self, m):
        def visit(z):
            for way, size in enumerate(self.totals(m, z)):
                if size:
                    self.all_of(m, way, size).wait_send()

        self.each_place(visit)


def gather_sems(total, parts, counts, large=None):
    dma = pltpu.SemaphoreType.DMA
    return [dma((len(counts), parts)), dma((len(counts),)), dma((len(counts), 4))] + [
        dma((total * count,)) for count in counts[:large]
    ]


def gather_kernel(depth, count, *refs):
    ins, slots = [(ref,) for ref in refs[:count]], refs[count : 2 * count]
    sems = refs[2 * count :]
    gather = Gather(depth, ins, slots, *sems[:3], sems[3:])
    gather.start_local()
    gather.barrier()
    gather.start_own(0)
    for m in range(count):
        gather.run(m)
    for m in range(count):
        gather.settle(m)
        gather.drain(m)


def gather_all(blocks):
    total = lax.axis_size("fs")
    count = len(blocks)
    outs = [jax.ShapeDtypeStruct((total * b.shape[0], *b.shape[1:]), b.dtype) for b in blocks]
    return pl.pallas_call(
        functools.partial(gather_kernel, total // 2, count),
        out_shape=outs,
        in_specs=[pl.BlockSpec(memory_space=pl.ANY)] * count,
        out_specs=[pl.BlockSpec(memory_space=pltpu.VMEM)] * count,
        scratch_shapes=gather_sems(total, 1, [b.shape[0] for b in blocks]),
        compiler_params=pltpu.CompilerParams(
            collective_id=0, has_side_effects=True, vmem_limit_bytes=48 * 2**20
        ),
        name="gather_all",
    )(*blocks)


def hidden_units(gathered, whole_gate, whole_up):
    gate_rows = jnp.dot(gathered, whole_gate, preferred_element_type=jnp.float32)
    up_rows = jnp.dot(gathered, whole_up, preferred_element_type=jnp.float32)
    return (jax.nn.silu(gate_rows) * up_rows).astype(jnp.bfloat16)


def columns_of(blocks):
    return blocks.transpose(1, 0, 2).reshape(blocks.shape[1], -1)


def causal_taps(glu, kernel):
    length = glu.shape[0]
    taps = kernel.shape[0]
    padded = jnp.pad(glu, ((taps - 1, 0), (0, 0)))
    output = jnp.zeros_like(glu)
    for tap_index in range(taps):
        output = output + padded[tap_index : tap_index + length] * kernel[tap_index]
    return output


def chunked(block, pieces):
    return block.reshape(pieces, block.shape[0] // pieces, block.shape[1])


class Layer:
    def __init__(self, gather, tokens, gains, taps, out, scratch):
        self.gather = gather
        self.out = out
        (
            self.own,
            self.stream,
            self.rows,
            self.hidden,
            self.partial,
            self.landed,
            self.padded,
            self.conv,
            self.sums,
            self.act,
            self.mixed,
            *self.packed,
            self.packed_taps,
            self.gains,
            self.gain,
            self.taps,
            self.own_sems,
            self.row_send,
            self.row_recv,
            self.part_send,
            self.part_recv,
            self.sum_send,
            self.sum_recv,
            self.out_sem,
        ) = scratch
        self.half, self.width = self.own.shape
        self.units = self.hidden.shape[1]
        self.total = gather.depth * 2
        self.piece = self.width // self.total
        self.blocks = self.half // ROW_BLOCK
        self.tp = lax.axis_index("tp")
        self.partner = {"tp": 1 - self.tp}
        self.mine = pl.multiple_of(self.tp * self.half, self.half)
        self.theirs = pl.multiple_of((1 - self.tp) * self.half, self.half)
        inputs = (tokens, *gains, taps)
        self.loads = [
            pltpu.make_async_copy(src, dst, self.own_sems.at[n])
            for n, (src, dst) in enumerate(zip(inputs, (self.own, *self.packed, self.packed_taps)))
        ]

    def expand(self):
        for n, packed in enumerate(self.packed):
            target = self.gain if n == 3 else self.gains.at[n]
            for j in range(packed.shape[0]):
                row = packed[j : j + 1, :].astype(jnp.float32)
                target[:, j * LANES : (j + 1) * LANES] = jnp.broadcast_to(row, (SUBLANES, LANES))
        for j in range(self.taps.shape[0]):
            row = self.packed_taps[j : j + 1, :].astype(jnp.float32)
            self.taps[j] = jnp.broadcast_to(row, (SUBLANES, row.shape[1]))

    def remote(self, src, dst, send_sem, recv_sem):
        return pltpu.make_async_remote_copy(
            src_ref=src,
            dst_ref=dst,
            send_sem=send_sem,
            recv_sem=recv_sem,
            device_id=self.partner,
            device_id_type=MESH,
        )

    def row_copy(self, n, first, count):
        here = self.rows.at[n, pl.ds(first, count)]
        return self.remote(here, here, self.row_send.at[n], self.row_recv.at[n])

    def await_rows(self, n):
        self.row_copy(n, self.theirs, self.half).wait_recv()

    def part_copy(self, n, k, width=None):
        cols = pl.ds(pl.multiple_of(k * self.piece, self.piece), self.piece if width is None else width)
        return self.remote(
            self.partial.at[n, pl.ds(self.theirs, self.half), cols],
            self.landed.at[n, :, cols],
            self.part_send.at[n],
            self.part_recv.at[n + (k if n == 2 else 0)],
        )

    def sum_copy(self):
        return self.remote(self.sums.at[0], self.sums.at[1], self.sum_send.at[0], self.sum_recv.at[0])

    def norm(self, n, i, stream):
        square_mean = jnp.mean(stream * stream, axis=-1, keepdims=True)
        scaled = (stream * lax.rsqrt(square_mean + ROW_EPS)).reshape(-1, SUBLANES, self.width) * self.gains[n][None]
        rows = pl.ds(self.mine + self.block(i), ROW_BLOCK)
        self.rows[n, rows, :] = scaled.reshape(stream.shape).astype(jnp.bfloat16)
        self.row_copy(n, self.mine + self.block(i), ROW_BLOCK).start()

    def block(self, i):
        return pl.multiple_of(i * ROW_BLOCK, ROW_BLOCK)

    def start_rows(self):
        def step(i, carry):
            self.norm(0, i, self.own[pl.ds(self.block(i), ROW_BLOCK), :].astype(jnp.float32))
            return carry

        lax.fori_loop(0, self.blocks, step, 0)

    def update(self, n, i, scale):
        first = self.block(i)
        here = pl.ds(first, ROW_BLOCK)
        before = self.own[here, :].astype(jnp.float32) if n == 0 else self.stream[here, :]
        added = self.partial[n, pl.ds(self.mine + first, ROW_BLOCK), :].astype(jnp.float32) + self.landed[
            n, here, :
        ].astype(jnp.float32)
        stream = before + (added if scale is None else scale * added)
        self.stream[here, :] = stream
        self.norm(n + 1, i, stream)

    def await_parts(self, n):
        self.part_copy(n, 0, self.width).wait_recv()

    def matrix(self, m, first, size):
        return self.gather.slots[m][:, :, pl.ds(first, size)].reshape(self.width, size)

    def columns(self, m, k):
        count = self.gather.count(m)
        return self.gather.slots[m][pl.ds(k * count, count)].reshape(-1, self.piece)

    def hidden_tile(self, n, row, height, first, size):
        rows = self.rows[n, pl.ds(row, height), :]
        gate = jnp.dot(rows, self.matrix(0, first, size), preferred_element_type=jnp.float32)
        up = jnp.dot(rows, self.matrix(1, first, size), preferred_element_type=jnp.float32)
        self.hidden[pl.ds(row, height), pl.ds(first, size)] = (jax.nn.silu(gate) * up).astype(jnp.bfloat16)

    def down_piece(self, n, k):
        weights = self.columns(2, k)
        result = jnp.dot(self.hidden[...], weights, preferred_element_type=jnp.float32)
        cols = pl.ds(pl.multiple_of(k * self.piece, self.piece), self.piece)
        self.partial[n, :, cols] = result.astype(jnp.bfloat16)
        self.part_copy(n, k).start()

    def first_work(self, t):
        j = t - FIRST_SLOT

        @pl.when(j == 0)
        def _():
            self.gather.settle(0)
            self.gather.settle(1)
            self.await_rows(0)

        @pl.when(jnp.logical_and(j >= 0, j < self.units // LANES))
        def _():
            self.hidden_tile(0, 0, 2 * self.half, pl.multiple_of(j * LANES, LANES), LANES)

    def second_work(self, t):
        pl.when(t == SECOND_SLOT)(lambda: self.gather.settle(2))

        def step(u, carry):
            j = (t - SECOND_SLOT) * PER_SLOT + u
            i = j - self.total
            pl.when(jnp.logical_and(j >= 0, i < 0))(lambda: self.down_piece(0, j))
            pl.when(i == 0)(lambda: self.await_parts(0))
            pl.when(jnp.logical_and(i >= 0, i < self.blocks))(lambda: self.update(0, i, 0.5))
            return carry

        lax.fori_loop(0, PER_SLOT, step, 0)

    def third_work(self, t):
        blocks = 2 * self.half // CONV_BLOCK

        def step(u, carry):
            j = (t - THIRD_SLOT) * PER_SLOT + u
            i = j - 2

            @pl.when(jnp.logical_or(j == 0, j == 1))
            def _():
                pl.when(j == 0)(lambda: self.gather.settle(3))
                pl.when(j == 1)(lambda: self.await_rows(1))
                self.gated(pl.multiple_of(jnp.where(j == 0, self.mine, self.theirs), self.half))

            pl.when(jnp.logical_and(i >= 0, i < blocks))(lambda: self.convolve(i))
            pl.when(i == blocks)(lambda: self.sum_copy().start())
            i = i - blocks - SUM_WAIT
            pl.when(i == 0)(lambda: self.sum_copy().wait_recv())
            pl.when(jnp.logical_and(i >= 0, i < blocks))(lambda: self.activate(i))
            return carry

        lax.fori_loop(0, PER_SLOT, step, 0)

    def gated(self, row):
        rows = self.rows[1, pl.ds(row, self.half), :]
        whole = self.gather.slots[3]
        height = whole.shape[1] // 2
        value = whole[:, :height, :].reshape(self.width, -1)
        gate = whole[:, height:, :].reshape(self.width, -1)
        values = jnp.dot(rows, value, preferred_element_type=jnp.float32)
        gates = jnp.dot(rows, gate, preferred_element_type=jnp.float32)
        self.padded[pl.ds(PAD + row, self.half), :] = values * jax.nn.sigmoid(gates)

    def convolve(self, i):
        taps = self.taps.shape[0]
        lanes = self.sums.shape[-1]
        first = pl.multiple_of(i * CONV_BLOCK, CONV_BLOCK)
        window = self.padded[pl.ds(first, CONV_BLOCK + PAD), :]
        channels = window.shape[1]
        total = jnp.zeros((CONV_BLOCK // SUBLANES, SUBLANES, channels), jnp.float32)
        offsets = [PAD - (taps - 1) + j for j in range(taps)]
        for shift in range(SUBLANES):
            mine = [(j, at) for j, at in enumerate(offsets) if at % SUBLANES == shift]
            reach = max(at for _, at in mine) - shift + CONV_BLOCK
            shifted = window[shift : shift + reach]
            for j, at in mine:
                block = shifted[at - shift : at - shift + CONV_BLOCK].reshape(total.shape)
                total = total + block * self.taps[j][None]
        total = total.reshape(CONV_BLOCK, channels)
        here = pl.ds(first, CONV_BLOCK)
        self.conv[here, :] = total
        plain = jnp.sum(total, axis=-1, keepdims=True)
        squared = jnp.sum(total * total, axis=-1, keepdims=True)
        lane = lax.broadcasted_iota(jnp.int32, (CONV_BLOCK, lanes), 1)
        self.sums[0, here, :] = jnp.where(lane < lanes // 2, plain, squared)

    def activate(self, i):
        lanes = self.sums.shape[-1]
        channels = 2 * self.conv.shape[1]
        here = pl.ds(pl.multiple_of(i * CONV_BLOCK, CONV_BLOCK), CONV_BLOCK)
        sums = (self.sums[0, here, :] + self.sums[1, here, :]) / channels
        average, square = sums[:, :1], sums[:, lanes // 2 : lanes // 2 + 1]
        spread = jnp.maximum(square - average * average, 0.0)
        scaled = (self.conv[here, :] - average) * lax.rsqrt(spread + CHAN_EPS)
        scaled = scaled.reshape(-1, SUBLANES, scaled.shape[1]) * self.gain[...][None]
        self.act[here, :] = jax.nn.silu(scaled.reshape(CONV_BLOCK, -1)).astype(jnp.bfloat16)

    def mix(self, row, k):
        rows, cols = pl.ds(row, self.half), pl.ds(pl.multiple_of(k * self.piece, self.piece), self.piece)
        result = jnp.dot(self.act[rows, :], self.columns(4, k), preferred_element_type=jnp.float32)
        self.partial[1, rows, cols] = result.astype(jnp.bfloat16)

    def finish_conv(self):
        self.gather.settle(4)

        def theirs(g, carry):
            group = [g * MIX_GROUP + u for u in range(MIX_GROUP)]
            for k in group:
                self.mix(self.theirs, k)
            for k in group:
                self.part_copy(1, k).start()
            return carry

        def mine(g, carry):
            for u in range(MIX_GROUP):
                self.mix(self.mine, g * MIX_GROUP + u)
            return carry

        lax.fori_loop(0, self.total // MIX_GROUP, theirs, 0)
        lax.fori_loop(0, self.total // MIX_GROUP, mine, 0)
        self.await_parts(1)

        def step(i, carry):
            self.update(1, i, None)
            return carry

        lax.fori_loop(0, self.blocks, step, 0)

    def second_half_step(self):
        tile = 2 * LANES
        whole = self.units // tile
        early = min(2, whole)

        def split(i, carry):
            pl.when(i == early)(lambda: self.await_rows(2))
            row = jnp.where(i < early, self.mine, self.theirs)
            first = pl.multiple_of(lax.rem(i, early) * tile, tile)
            self.hidden_tile(2, pl.multiple_of(row, self.half), self.half, first, tile)
            return carry

        lax.fori_loop(0, 2 * early, split, 0)

        def step(j, carry):
            self.hidden_tile(2, 0, 2 * self.half, pl.multiple_of(j * tile, tile), tile)
            return carry

        lax.fori_loop(early, whole, step, 0)
        if self.units % tile:
            self.hidden_tile(2, 0, 2 * self.half, whole * tile, self.units % tile)

        def down(row, k):
            return jnp.dot(self.hidden[pl.ds(row, self.half), :], self.columns(2, k), preferred_element_type=jnp.float32)

        def columns(k):
            return pl.ds(pl.multiple_of(k * self.piece, self.piece), self.piece)

        def theirs(g, carry):
            group = [g * DOWN_GROUP + u for u in range(DOWN_GROUP)]
            for k in group:
                self.partial[2, pl.ds(self.theirs, self.half), columns(k)] = down(self.theirs, k).astype(jnp.bfloat16)
            for k in group:
                self.part_copy(2, k).start()
            return carry

        def mine(g, carry):
            group = [g * DOWN_GROUP + u for u in range(DOWN_GROUP)]
            for k in group:
                self.part_copy(2, k).wait_recv()
            for k in group:
                cols = columns(k)
                own = down(self.mine, k).astype(jnp.bfloat16).astype(jnp.float32)
                added = own + self.landed[2, :, cols].astype(jnp.float32)
                self.mixed[:, cols] = (self.stream[:, cols] + 0.5 * added).astype(self.mixed.dtype)
            for k in group:
                cols = columns(k)
                pltpu.make_async_copy(self.mixed.at[:, cols], self.out.at[:, cols], self.out_sem.at[0]).start()
            return carry

        lax.fori_loop(0, self.total // DOWN_GROUP, theirs, 0)
        lax.fori_loop(0, self.total // DOWN_GROUP, mine, 0)

    def drain(self):
        self.sum_copy().wait_send()
        for n in range(3):
            self.row_copy(n, self.mine, self.half).wait_send()
            self.part_copy(n, 0, self.width).wait_send()

    def run(self):
        gather = self.gather
        gather.start_local()
        for load in self.loads:
            load.start()
        gather.barrier(self.partner)
        gather.start_own(0)
        for load in self.loads:
            load.wait()
        self.expand()
        self.start_rows()
        self.padded[:PAD, :] = jnp.zeros((PAD, self.padded.shape[1]), jnp.float32)
        gather.run(0)
        gather.run(1)
        gather.run(2, self.first_work)
        gather.run(3, self.second_work)
        gather.run(4, self.third_work)
        self.finish_conv()
        self.second_half_step()
        for m in range(len(gather.ins)):
            gather.drain(m)
        self.drain()
        pltpu.make_async_copy(self.mixed, self.out, self.out_sem.at[0]).wait()


def layer_kernel(depth, *refs):
    tokens, gains, taps, refs = refs[0], refs[1:5], refs[5], refs[6:]
    ins, refs = ((refs[0],), (refs[1],), (refs[2],), refs[3:5], (refs[5],)), refs[6:]
    out, refs = refs[0], refs[1:]
    slots, sems, scratch = refs[:5], refs[5:11], refs[11:]
    gather = Gather(depth, ins, slots, *sems[:3], (*sems[3:], *sems[3:5]))
    Layer(gather, tokens, gains, taps, out, scratch).run()


def fused_layer(tokens, gains, depthwise, blocks, smalls):
    total = lax.axis_size("fs")
    half, width = tokens.shape
    units, (taps, channels) = blocks[0].shape[2], depthwise.shape
    vmem, dma = pltpu.VMEM, pltpu.SemaphoreType.DMA
    count, height, piece = smalls[0].shape
    shapes = [b.shape for b in blocks] + [(count, 2 * height, piece), (count, height, piece)]
    f32, bf16 = jnp.float32, jnp.bfloat16
    return pl.pallas_call(
        functools.partial(layer_kernel, total // 2),
        out_shape=jax.ShapeDtypeStruct((half, width), bf16),
        in_specs=[pl.BlockSpec(memory_space=pltpu.HBM)] * 12,
        out_specs=pl.BlockSpec(memory_space=pltpu.HBM),
        scratch_shapes=[vmem((total * shape[0], *shape[1:]), bf16) for shape in shapes]
        + gather_sems(total, 2, [shape[0] for shape in shapes], LARGE)
        + [
            vmem((half, width), bf16),
            vmem((half, width), f32),
            vmem((3, 2 * half, width), bf16),
            vmem((2 * half, units), bf16),
            vmem((3, 2 * half, width), bf16),
            vmem((3, half, width), bf16),
            vmem((PAD + 2 * half, channels), f32),
            vmem((2 * half, channels), f32),
            vmem((2, 2 * half, LANES), f32),
            vmem((2 * half, channels), bf16),
            vmem((half, width), bf16),
        ]
        + [vmem(gain.shape, bf16) for gain in gains]
        + [
            vmem(depthwise.shape, bf16),
            vmem((3, SUBLANES, width), f32),
            vmem((SUBLANES, channels), f32),
            vmem((taps, SUBLANES, channels), f32),
            dma((6,)),
            dma((3,)),
            dma((3,)),
            dma((3,)),
            dma((2 + total,)),
            dma((1,)),
            dma((1,)),
            dma((1,)),
        ],
        compiler_params=pltpu.CompilerParams(
            collective_id=0, has_side_effects=True, vmem_limit_bytes=58 * 2**20
        ),
        name="fused_layer",
    )(tokens, *gains, depthwise, *blocks, *smalls)


def fits(half, ffn_gate, ffn_down, conv_value, conv_out, depthwise):
    piece, total = ffn_gate.shape[0], lax.axis_size("fs")
    slots, conv_slots = total // 2 * CHUNKS, total // 2 * CONV_CHUNKS
    return (
        piece % (16 * CHUNKS) == 0
        and ffn_down.shape[0] % (16 * CHUNKS) == 0
        and conv_out.shape[0] == piece
        and conv_value.shape[1] == piece
        and piece % LANES == 0
        and ffn_gate.shape[1] % LANES == 0
        and half % ROW_BLOCK == 0
        and half % CONV_BLOCK == 0
        and depthwise.shape[0] <= PAD
        and total % MIX_GROUP == 0
        and total % DOWN_GROUP == 0
        and slots >= FIRST_SLOT + ffn_gate.shape[1] // LANES
        and (conv_slots - SECOND_SLOT) * PER_SLOT >= total + half // ROW_BLOCK
        and (conv_slots - THIRD_SLOT) * PER_SLOT >= 2 + SUM_WAIT + 4 * half // CONV_BLOCK
        and lax.axis_size("tp") == 2
        and lax.axis_size("rep") == 2
    )


def shards(
    tokens,
    norm_first,
    norm_mixer,
    norm_second,
    ffn_gate,
    ffn_up,
    ffn_down,
    conv_value,
    conv_gate,
    depthwise,
    conv_gain,
    conv_out,
):
    width = tokens.shape[-1]
    if fits(tokens.size // width, ffn_gate, ffn_down, conv_value, conv_out, depthwise):
        mixed = fused_layer(
            tokens.reshape(-1, width),
            [gain.reshape(-1, LANES) for gain in (norm_first, norm_mixer, norm_second, conv_gain)],
            depthwise,
            [chunked(block, CHUNKS) for block in (ffn_gate, ffn_up, ffn_down)],
            [chunked(block, CONV_CHUNKS) for block in (conv_value, conv_gate, conv_out)],
        )
        return mixed.reshape(tokens.shape)
    stream = tokens.reshape(-1, width).astype(jnp.float32)
    first_rows = widen(rms_rows(stream, norm_first))
    small = jnp.concatenate([conv_value, conv_gate, conv_out.reshape(-1, conv_value.shape[1])])
    gate, up, down, small_all = gather_all(
        [chunked(block, CHUNKS) for block in (ffn_gate, ffn_up, ffn_down, small)]
    )
    whole_gate = gate.reshape(-1, gate.shape[-1])
    whole_up = up.reshape(-1, up.shape[-1])
    total = lax.axis_size("fs")
    whole_down = columns_of(down.reshape(total, -1, down.shape[-1]))
    small_all = small_all.reshape(total, -1, small_all.shape[-1])
    rows = conv_value.shape[0]
    channels_here = conv_value.shape[1]
    whole_value = small_all[:, :rows].reshape(-1, channels_here)
    whole_conv_gate = small_all[:, rows : 2 * rows].reshape(-1, channels_here)
    whole_out = columns_of(small_all[:, 2 * rows :].reshape(total, *conv_out.shape))

    hidden = hidden_units(first_rows, whole_gate, whole_up)
    stream = stream + 0.5 * narrow(jnp.dot(hidden, whole_down, preferred_element_type=jnp.float32))
    gathered = widen(rms_rows(stream, norm_mixer))
    values = jnp.dot(gathered, whole_value, preferred_element_type=jnp.float32)
    gates = jnp.dot(gathered, whole_conv_gate, preferred_element_type=jnp.float32)
    glu = reorder(values * jax.nn.sigmoid(gates))
    conv = causal_taps(glu, depthwise.astype(jnp.float32))
    channels = conv.shape[1] * lax.axis_size("tp")
    sums, squares = lax.psum((jnp.sum(conv, axis=1), jnp.sum(conv * conv, axis=1)), "tp")
    average = sums / channels
    spread = jnp.maximum(squares / channels - average * average, 0.0)
    centred = conv - average[:, None]
    activated = jax.nn.silu(
        centred * lax.rsqrt(spread[:, None] + CHAN_EPS) * conv_gain.astype(jnp.float32)
    ).astype(jnp.bfloat16)
    stream = stream + narrow(jnp.dot(reorder(activated), whole_out, preferred_element_type=jnp.float32))
    second_rows = widen(rms_rows(stream, norm_second))
    second_hidden = hidden_units(second_rows, whole_gate, whole_up)
    stream = stream + 0.5 * narrow(jnp.dot(second_hidden, whole_down, preferred_element_type=jnp.float32))
    return stream.astype(jnp.bfloat16).reshape(tokens.shape)


def solution(mesh):
    in_specs = (
        P(("rep", "fs"), "tp", None),
        P(),
        P(),
        P(),
        P("fs", "tp"),
        P("fs", "tp"),
        P("tp", "fs"),
        P("fs", "tp"),
        P("fs", "tp"),
        P(None, "tp"),
        P("tp"),
        P("tp", "fs"),
    )
    out_specs = P(("rep", "fs"), "tp", None)
    return jax.shard_map(shards, mesh=mesh, in_specs=in_specs, out_specs=out_specs, check_vma=False)
```
